128 devices in a mesh: kv: 16 (over z, y), tp: 8 (over x, core).
Axes of the slice: x: 4, y: 4, z: 4, core: 2. Of those that a mesh axis runs over, the one named last changes fastest.
Arguments:
- tokens: bfloat16 [32, 4096], P(None, 'kv'), may hold values from -40 to 40, as said below
- norm_gain: float32 [4096], P('kv'), may hold values from 0.1 to 1.9
- w_query: bfloat16 [4096, 2048], P('kv', 'tp'), may hold values from -0.09375 to 0.09375
- w_key: bfloat16 [4096, 512], P('kv', 'tp'), may hold values from -0.09375 to 0.09375
- w_value: bfloat16 [4096, 512], P('kv', 'tp'), may hold values from -0.09375 to 0.09375
- forget_weight: bfloat16 [4096, 32], replicated, may hold values from -0.09375 to 0.09375
- forget_bias: float32 [32], P('tp'), may hold values from -1 to 3
- kv_cache: bfloat16 [32, 20480, 8, 128], P(None, 'kv', 'tp'), may hold values from -6 to 6
- cum_gates: float32 [32, 32, 20480], P(None, 'tp', 'kv'), may hold values from -20740 to 0, as said below
- lengths: int32 [32], replicated, may hold values from 1 to 20480, as said below
- w_out: bfloat16 [2048, 4096], P('tp', 'kv'), may hold values from -0.25 to 0.25
Outputs:
- mixed: bfloat16 [32, 4096], P(None, 'kv')
- log_weight: float32 [32, 32], P(None, 'tp')
The draws below stay inside these ranges and needn't reach their ends.
Inputs may be any that keep to these rules, and one draw needn't show every extreme that they name: Columns of tokens come in 16 groups of equal width. `cum_gates`: each row does not rise along the positions. `lengths`: some sequence has all 20480 positions cached.
All inputs are finite; a program needn't handle non-finite values.
Results may differ from the reference program's by a relative error of at most 0.0307.
Values may be sent and summed in bfloat16 or wider, within the bound.
A program may use at most 64 MiB of HBM per device.

```python
import math
import jax
import jax.numpy as jnp
from jax import lax

D = 4096
HEADS = 32
KV_HEADS = 8
HEAD = 64
BATCH = 32
CTX_DEV = 1280
LENGTH = 20480
N_KV = 16
N_TP = 8


def draw_tokens(key, part):
    first_key, second_key, third_key = jax.random.split(key, 3)
    base = jax.random.normal(first_key, (BATCH, D), jnp.float32)
    group_scale = jnp.exp(jax.random.uniform(second_key, (16,), jnp.float32, math.log(0.3), math.log(3.0)))
    columns = jnp.repeat(group_scale, D // 16)
    values = base * columns
    return jnp.clip(values, -40.0, 40.0).astype(jnp.bfloat16)


def draw_cum_gates(key, part):
    first_key, second_key, third_key = jax.random.split(key, 3)
    shift_key = jax.random.fold_in(key, 11)
    pick_key, depth_key, forced_key = jax.random.split(shift_key, 3)
    fast_share = 0.5
    is_fast = jax.random.uniform(first_key, (BATCH, HEADS), jnp.float32) < fast_share
    rate = jnp.where(is_fast, 1.0 / 30.0, 1.0 / LENGTH)
    block_factor = jnp.exp(jax.random.uniform(second_key, (BATCH, HEADS, LENGTH // CTX_DEV), jnp.float32, math.log(0.35), math.log(2.8)))
    block_factor = jnp.repeat(block_factor, CTX_DEV, axis=2)
    step_size = jax.random.uniform(third_key, (BATCH, HEADS, LENGTH), jnp.float32, 0.2, 1.8)
    log_forget = -rate[:, :, None] * block_factor * step_size
    shifted = jax.random.uniform(pick_key, (BATCH, HEADS), jnp.float32) < 0.25
    depth = jax.random.uniform(depth_key, (BATCH, HEADS), jnp.float32, 120.0, 260.0)
    forced = jax.random.randint(forced_key, (), 0, BATCH * HEADS)
    flat_index = jnp.arange(BATCH * HEADS, dtype=jnp.int32).reshape(BATCH, HEADS)
    offset = jnp.where(shifted, -depth, 0.0)
    offset = jnp.where(flat_index == forced, -jnp.maximum(depth, 200.0), offset)
    return jnp.cumsum(log_forget, axis=2) + offset[:, :, None]


def draw_lengths(key, part):
    first_key, second_key = jax.random.split(key)
    values = jax.random.randint(first_key, (BATCH,), 1, LENGTH + 1).astype(jnp.int32)
    chosen = jax.random.randint(second_key, (), 0, BATCH)
    return values.at[chosen].set(LENGTH).astype(jnp.int32)


def level_of(key, shape, cuts, low, largest):
    gain = 1.0
    for axis_at, blocks in cuts:
        draws = jax.random.uniform(jax.random.fold_in(jax.random.fold_in(key, 6), axis_at), (blocks,), jnp.float32, low / len(cuts), largest / len(cuts))
        gain = gain * jnp.repeat(jnp.exp(draws), shape[axis_at] // blocks).reshape((-1,) + (1,) * (len(shape) - 1 - axis_at))
    return gain


def noise(rng, dims, scale, most, cuts=(), kind=jnp.bfloat16):
    entries = jax.random.normal(rng, dims, jnp.float32) * scale
    if len(cuts) > 0:
        entries = level_of(rng, dims, cuts, -0.22, 0.18) * entries
    return jnp.clip(entries, min=-most, max=most).astype(kind)


def setup_inputs(seed: int = 0) -> dict:
    key_list = jax.random.split(jax.random.key(seed), 12)
    tokens = draw_tokens(jax.random.fold_in(key_list[11], 71), 0)
    norm_gain = jnp.clip(1.0 + 0.18 * jax.random.normal(key_list[1], (D,), jnp.float32), 0.1, 1.9)
    w_query = noise(key_list[2], (D, HEADS * HEAD), D ** -0.5, 0.09375, ((0, 16), (1, 8)))
    w_key = noise(key_list[3], (D, KV_HEADS * HEAD), D ** -0.5, 0.09375, ((0, 16), (1, 8)))
    w_value = noise(key_list[4], (D, KV_HEADS * HEAD), D ** -0.5, 0.09375, ((0, 16), (1, 8)))
    forget_weight = noise(key_list[5], (D, HEADS), D ** -0.5, 0.09375)
    forget_bias = jnp.clip(-1.0 + 4.0 * jax.random.uniform(key_list[6], (HEADS,), jnp.float32) ** level_of(key_list[6], (HEADS,), ((0, 8),), -0.2, 0.2), -1.0, 3.0)
    kv_cache = noise(key_list[7], (BATCH, LENGTH, KV_HEADS, 2 * HEAD), 1.0, 6.0, ((1, 16), (2, 8)))
    cum_gates = draw_cum_gates(jax.random.fold_in(key_list[11], 71), 0)
    lengths = draw_lengths(jax.random.fold_in(key_list[11], 71), 0)
    w_out = noise(key_list[10], (HEADS * HEAD, D), (HEAD * 8) ** -0.5, 0.25, ((0, 8), (1, 16)))
    return dict(tokens=tokens, norm_gain=norm_gain, w_query=w_query, w_key=w_key, w_value=w_value, forget_weight=forget_weight, forget_bias=forget_bias, kv_cache=kv_cache, cum_gates=cum_gates, lengths=lengths, w_out=w_out)


norm_eps = 1e-05
masked_floor = -1e+30

def reference(tokens, norm_gain, w_query, w_key, w_value, forget_weight, forget_bias, kv_cache, cum_gates, lengths, w_out):
    tokens_f = tokens.astype(jnp.float32)
    row_scale = lax.rsqrt(lax.optimization_barrier(jnp.mean(tokens_f * tokens_f, axis=1)) + norm_eps)[:, None]
    normalized_input = (tokens_f * norm_gain).astype(jnp.bfloat16)
    query = (row_scale * jnp.dot(normalized_input, w_query, preferred_element_type=jnp.float32)).astype(jnp.bfloat16)
    fresh_key_row = (row_scale * jnp.dot(normalized_input, w_key, preferred_element_type=jnp.float32)).astype(jnp.bfloat16)
    value_new = (row_scale * jnp.dot(normalized_input, w_value, preferred_element_type=jnp.float32)).astype(jnp.bfloat16)
    log_gate = jax.nn.log_sigmoid(row_scale * jnp.dot(normalized_input, forget_weight, preferred_element_type=jnp.float32) + forget_bias)
    group_size = HEADS // KV_HEADS
    inv_root = HEAD ** (-0.5)

    def one_row(items):
        query_row, key_row, value_row, forget_gate_row, cache_row, cum_row, length = items
        query_head_rows = query_row.astype(jnp.float32).reshape(KV_HEADS, group_size, HEAD)
        cached_keys = cache_row[:, :, :HEAD].astype(jnp.float32)
        cached_vals = cache_row[:, :, HEAD:].astype(jnp.float32)
        scores = jnp.einsum('kgd,lkd->kgl', query_head_rows, cached_keys) * inv_root
        biased = scores - cum_row.reshape(KV_HEADS, group_size, LENGTH)
        last_cum = lax.dynamic_index_in_dim(cum_row, (length - 1).astype(jnp.int32), axis=1, keepdims=False)
        cum_query = last_cum + forget_gate_row
        key_heads = key_row.astype(jnp.float32).reshape(KV_HEADS, HEAD)
        new_biased = jnp.einsum('kgd,kd->kg', query_head_rows, key_heads) * inv_root - cum_query.reshape(KV_HEADS, group_size)
        blocked = biased.reshape(KV_HEADS, group_size, N_KV, CTX_DEV)
        in_range = (jnp.arange(LENGTH, dtype=jnp.int32) < length).reshape(N_KV, CTX_DEV)
        holds_last = jnp.arange(N_KV, dtype=jnp.int32) == (length - 1) // CTX_DEV
        block_peak = lax.optimization_barrier(jnp.max(jnp.where(in_range, blocked, masked_floor), axis=-1))
        block_peak = jnp.where(holds_last, jnp.maximum(block_peak, new_biased[..., None]), block_peak)
        weights = jnp.where(in_range, jnp.exp(blocked - block_peak[..., None]), 0.0)
        new_weight = jnp.where(holds_last, jnp.exp(new_biased[..., None] - block_peak), 0.0)
        block_sum = lax.optimization_barrier(jnp.sum(weights, axis=-1)) + new_weight
        rounded = lax.optimization_barrier(weights.astype(jnp.bfloat16)).astype(jnp.float32)
        rounded_new = lax.optimization_barrier(new_weight.astype(jnp.bfloat16)).astype(jnp.float32)
        value_block_rows = jnp.einsum('kgnl,nlkd->kgnd', rounded, cached_vals.reshape(N_KV, CTX_DEV, KV_HEADS, HEAD))
        value_heads = value_row.astype(jnp.float32).reshape(KV_HEADS, 1, 1, HEAD)
        value_block_rows = value_block_rows + rounded_new[..., None] * value_heads
        peak = lax.optimization_barrier(jnp.max(block_peak, axis=-1))
        rescale_factor = jnp.exp(block_peak - peak[..., None])
        weight_sum = lax.optimization_barrier(jnp.sum(block_sum * rescale_factor, axis=-1))
        values = lax.optimization_barrier(jnp.sum(value_block_rows * rescale_factor[..., None], axis=2))
        attended = (values / weight_sum[..., None]).astype(jnp.bfloat16).reshape(HEADS * HEAD)
        log_weight = (peak + jnp.log(weight_sum)).reshape(HEADS) + cum_query
        return (attended, log_weight)
    attended, log_weight = lax.map(one_row, (query, fresh_key_row, value_new, log_gate, kv_cache, cum_gates, lengths))
    group_cols = HEADS * HEAD // N_TP
    pieces = attended.astype(jnp.float32).reshape(BATCH, N_TP, group_cols)
    out_rows = w_out.astype(jnp.float32).reshape(N_TP, group_cols, D)
    partial_out = jnp.einsum('bgc,gcd->gbd', pieces, out_rows).astype(jnp.bfloat16)
    partial_out = lax.optimization_barrier(partial_out)
    mixed = lax.optimization_barrier(jnp.sum(partial_out.astype(jnp.float32), axis=0)).astype(jnp.bfloat16)
    return (mixed, log_weight)
```

```python
import functools
import itertools

import jax
import jax.numpy as jnp
from jax import lax
from jax.experimental import pallas as pl
from jax.experimental.pallas import tpu as pltpu
from jax.sharding import Mesh
from jax.sharding import PartitionSpec as P

KV = ("kv_0", "kv_1")
ORDERS = (("kv_1", "kv_0"), ("kv_0", "kv_1"))
MESH = pl.DeviceIdType.MESH
NT = (((1,), (1,)), ((), ()))
norm_eps = 1e-05
masked_floor = -1e30
empty_peak = -1e29
f32, bf16 = jnp.float32, jnp.bfloat16


def iota(shape, axis):
    return lax.broadcasted_iota(jnp.int32, shape, axis)


def kernel(
    n_kv0,
    n_kv1,
    n_tp,
    tokens,
    gain,
    w_query,
    w_key,
    w_value,
    gate_rows,
    gate_bias,
    cache,
    cum,
    lengths,
    w_out,
    mixed,
    log_weight,
    tok_v,
    gain_v,
    wq_v,
    wkv_v,
    wg_v,
    wo_v,
    cache_v,
    cum_v,
    keys_t,
    cum_neg,
    biased,
    weights,
    qg_1,
    qg_2,
    new_1,
    new_2,
    val_1,
    val_2,
    stat_1,
    stat_2,
    out_x,
    load_sem,
    send_sem,
    recv_sem,
):
    place = {"kv_0": lax.axis_index("kv_0"), "kv_1": lax.axis_index("kv_1"), "tp": lax.axis_index("tp")}
    sizes = {"kv_0": n_kv0, "kv_1": n_kv1, "tp": n_tp}
    kv_index = place["kv_0"] * n_kv1 + place["kv_1"]
    batch, span = cache.shape[0], cache.shape[1]
    cols = tokens.shape[1]
    heads = cum.shape[1]
    head = cache.shape[2] // 2
    rows = heads * batch
    half = batch // 2
    width = cols * n_kv0 * n_kv1

    count = itertools.count()

    def load(src, dst):
        copy = pltpu.make_async_copy(src, dst, load_sem.at[next(count)])
        copy.start()
        return copy

    small = [
        load(tokens, tok_v),
        load(gain, gain_v),
        load(w_query, wq_v),
        load(w_key, wkv_v.at[pl.ds(0, head)]),
        load(w_value, wkv_v.at[pl.ds(head, head)]),
        load(gate_rows.at[:, pl.ds(pl.multiple_of(kv_index * cols, cols), cols)], wg_v.at[pl.ds(0, gate_rows.shape[0])]),
    ]
    cum_load = load(cum, cum_v)
    block = batch // 8
    cache_loads = [load(cache.at[pl.ds(k * block, block)], cache_v.at[pl.ds(k * block, block)]) for k in range(8)]
    wo_load = load(w_out, wo_v)

    barrier = pltpu.get_barrier_semaphore()
    for axis, size in sizes.items():
        for step in range(1, size):
            pl.semaphore_signal(
                barrier, inc=1, device_id={axis: lax.rem(place[axis] + step, size)}, device_id_type=MESH
            )

    numbers = itertools.count()
    sent = []

    def exchange(buffer, axis):
        size = sizes[axis]
        me = place[axis]
        waits = []
        for step in sorted(range(1, size), key=lambda s: -min(s, size - s)):
            number = next(numbers)
            source = lax.rem(me + size - step, size)
            out = pltpu.make_async_remote_copy(
                src_ref=buffer.at[me],
                dst_ref=buffer.at[me],
                send_sem=send_sem.at[number],
                recv_sem=recv_sem.at[number],
                device_id={axis: lax.rem(me + step, size)},
                device_id_type=MESH,
            )
            out.start()
            sent.append(out)
            waits.append(
                pltpu.make_async_remote_copy(
                    src_ref=buffer.at[source],
                    dst_ref=buffer.at[source],
                    send_sem=send_sem.at[number],
                    recv_sem=recv_sem.at[number],
                    device_id={axis: source},
                    device_id_type=MESH,
                )
            )
        return waits

    def arrived(waits):
        for wait in waits:
            wait.wait_recv()

    def total(buffer, size):
        acc = buffer[0].astype(f32)
        for k in range(1, size):
            acc = acc + buffer[k].astype(f32)
        return acc

    wg_v[gate_rows.shape[0] :, :] = jnp.zeros((wg_v.shape[0] - gate_rows.shape[0], cols), bf16)
    for copy in small:
        copy.wait()
    tokens_f = tok_v[...].astype(f32)
    squares = jnp.sum(tokens_f * tokens_f, axis=1, keepdims=True)
    normed = (tokens_f * gain_v[...]).astype(bf16)
    part_query = jnp.dot(normed, wq_v[...], preferred_element_type=f32).astype(bf16)
    part_gate = lax.dot_general(normed, wg_v[...], NT, preferred_element_type=f32)
    n_gates = gate_rows.shape[0]
    lane = iota((batch, 128), 1)
    part_gate = jnp.where(lane < n_gates, part_gate, squares).astype(bf16)
    part_new = lax.dot_general(normed, wkv_v[...], NT, preferred_element_type=f32).astype(bf16)
    for part in range(2):
        me = place[ORDERS[part][0]]
        chunk = slice(part * half, (part + 1) * half)
        qg_1[part, me, :, : heads * head] = part_query[chunk]
        qg_1[part, me, :, heads * head :] = part_gate[chunk]
        new_1[part, me] = part_new[chunk]

    pl.semaphore_wait(barrier, sum(size - 1 for size in sizes.values()))
    qg_waits = [exchange(qg_1.at[part], ORDERS[part][0]) for part in range(2)]
    new_waits = [exchange(new_1.at[part], ORDERS[part][0]) for part in range(2)]

    cum_load.wait()
    first_pos = kv_index * span
    length_rows = jnp.zeros((batch, 128), jnp.int32)
    for b in range(batch):
        length_rows = jnp.where(iota((batch, 128), 0) == b, lengths[b], length_rows)
    length_col = length_rows[:, :1] - first_pos
    last_parts = []
    for h in range(heads):
        last = jnp.zeros((batch, 128), f32)
        for n in range(span // 128):
            position = iota((batch, 128), 1) + n * 128
            value = cum_v[:, h, n * 128 : (n + 1) * 128]
            cum_neg[h * batch : (h + 1) * batch, n * 128 : (n + 1) * 128] = jnp.where(
                position < length_col, -value, masked_floor
            )
            last = last + jnp.where(position == length_col - 1, value, 0.0)
        last_parts.append(jnp.sum(last, axis=1, keepdims=True))
    last_cum = jnp.concatenate(last_parts, axis=0)
    holds = (length_col > 0) & (length_col <= span)
    holds = jnp.concatenate([jnp.where(holds, 1, 0)] * heads, axis=0) > 0

    def transpose_keys(first, count):
        def one(b, carry):
            flipped = cache_v[b].T
            keys_t[pl.ds(pl.multiple_of(b * head, head), head), :] = flipped[:head]
            return carry

        lax.fori_loop(first, first + count, one, 0)

    for part in range(2):
        arrived(qg_waits[part])
        me = place[ORDERS[part][1]]
        qg_2[part, me] = total(qg_1.at[part], sizes[ORDERS[part][0]]).astype(bf16)
    qg_waits = [exchange(qg_2.at[part], ORDERS[part][1]) for part in range(2)]
    for part in range(2):
        arrived(new_waits[part])
        me = place[ORDERS[part][1]]
        new_2[part, me] = total(new_1.at[part], sizes[ORDERS[part][0]]).astype(bf16)
    new_waits = [exchange(new_2.at[part], ORDERS[part][1]) for part in range(2)]

    for copy in cache_loads:
        copy.wait()
    transpose_keys(0, batch)

    for part in range(2):
        arrived(qg_waits[part])
    sums = jnp.concatenate([total(qg_2.at[part], sizes[ORDERS[part][1]]) for part in range(2)], axis=0)
    gates = sums[:, heads * head :]
    row_scale = lax.rsqrt(gates[:, n_gates : n_gates + 1] / width + norm_eps)
    query = (row_scale * sums[:, : heads * head]).astype(bf16).astype(f32)
    first_gate = place["tp"] * heads
    log_gate = []
    for h in range(heads):
        logit = jnp.sum(jnp.where(lane == first_gate + h, gates, 0.0), axis=1, keepdims=True)
        logit = row_scale * logit + gate_bias[h]
        log_gate.append(jnp.minimum(logit, 0.0) - jnp.log1p(jnp.exp(-jnp.abs(logit))))
    cum_query = last_cum + jnp.concatenate(log_gate, axis=0)

    doubled = []
    for pair in range(heads // 2):
        two = query[:, pair * 128 : (pair + 1) * 128]
        turned = pltpu.roll(two, 64, 1)
        doubled.append(jnp.where(lane < head, two, turned))
        doubled.append(jnp.where(lane < head, turned, two))
    doubled = jnp.concatenate(doubled, axis=0)
    row_of = iota((rows, 128), 0) % batch
    lane_of = iota((rows, 128), 1)
    side = jnp.where(lane_of < head, 0, 1)
    inv_root = head ** (-0.5)
    scaled = doubled * inv_root
    spread = jnp.concatenate(
        [jnp.where(row_of == 2 * p + side, scaled, 0.0).astype(bf16) for p in range(batch // 2)], axis=1
    )

    tile = 256
    peak = jnp.full((rows, 128), masked_floor, f32)
    for n in range(span // tile):
        cut = slice(n * tile, (n + 1) * tile)
        score = jnp.dot(spread, keys_t[:, cut], preferred_element_type=f32) + cum_neg[:, cut]
        biased[:, cut] = score
        for k in range(tile // 128):
            peak = jnp.maximum(peak, score[:, k * 128 : (k + 1) * 128])

    for part in range(2):
        arrived(new_waits[part])
    new_rows = jnp.concatenate([total(new_2.at[part], sizes[ORDERS[part][1]]) for part in range(2)], axis=0)
    new_rows = (row_scale * new_rows).astype(bf16).astype(f32)
    new_rows = jnp.concatenate([new_rows] * heads, axis=0)
    new_biased = (
        jnp.sum(jnp.where(lane_of < head, doubled * new_rows, 0.0), axis=1, keepdims=True) * inv_root
        - cum_query
    )

    peak = jnp.max(peak, axis=1, keepdims=True)
    peak = jnp.where(holds, jnp.maximum(peak, new_biased), peak)
    peak = jnp.maximum(peak, empty_peak)
    sums = jnp.zeros((rows, 128), f32)
    for n in range(span // 128):
        cut = slice(n * 128, (n + 1) * 128)
        weight = jnp.exp(biased[:, cut] - peak)
        sums = sums + weight
        weights[:, cut] = weight.astype(bf16)
    new_weight = jnp.where(holds, jnp.exp(new_biased - peak), 0.0)
    weight_sum = jnp.sum(sums, axis=1, keepdims=True) + new_weight

    values = new_weight.astype(bf16).astype(f32) * new_rows
    for p in range(batch // 2):
        both = jnp.concatenate([cache_v[2 * p], cache_v[2 * p + 1]], axis=1)
        out = jnp.dot(weights[...], both, preferred_element_type=f32)
        values = (
            values
            + jnp.where(row_of == 2 * p, out[:, :128], 0.0)
            + jnp.where(row_of == 2 * p + 1, out[:, 128:], 0.0)
        )

    diagonal = iota((rows, 128), 0) == lane_of

    def as_row(column):
        return jnp.sum(jnp.where(diagonal, column, 0.0), axis=0, keepdims=True)

    sub = iota((8, 128), 0)
    anchor = jnp.where(holds, cum_query, 0.0)
    stats = jnp.where(sub == 0, as_row(peak), jnp.where(sub == 1, as_row(weight_sum), as_row(anchor)))
    for part in range(2):
        me = place[ORDERS[part][0]]
        low = values[2 * part * batch : (2 * part + 1) * batch]
        high = values[(2 * part + 1) * batch : (2 * part + 2) * batch]
        val_1[part, me] = jnp.where(lane < head, pltpu.roll(low, 64, 1), high).astype(bf16)
        stat_1[part, me] = stats
    stat_waits = [exchange(stat_1.at[part], ORDERS[part][0]) for part in range(2)]
    val_waits = [exchange(val_1.at[part], ORDERS[part][0]) for part in range(2)]

    def combined(part, vals, stat, size, final):
        found = [stat[k] for k in range(size)]
        peak = functools.reduce(jnp.maximum, [s[0:1] for s in found])
        factors = [jnp.exp(s[0:1] - peak) for s in found]
        weight_sum = sum(s[1:2] * f for s, f in zip(found, factors))
        anchor = sum(s[2:3] for s in found)
        if final:
            factors = [f / weight_sum for f in factors]
        table = jnp.zeros((8, 128), f32)
        for k, f in enumerate(factors):
            table = jnp.where(sub == k, f, table)
        columns = table.T
        acc = None
        for k in range(size):
            low = columns[2 * part * batch : (2 * part + 1) * batch, k : k + 1]
            high = columns[(2 * part + 1) * batch : (2 * part + 2) * batch, k : k + 1]
            term = vals[k].astype(f32) * jnp.where(lane < head, low, high)
            acc = term if acc is None else acc + term
        return peak, weight_sum, anchor, acc

    for part in range(2):
        arrived(stat_waits[part])
        arrived(val_waits[part])
        first, second = ORDERS[part]
        peak, weight_sum, anchor, acc = combined(part, val_1.at[part], stat_1.at[part], sizes[first], False)
        me = place[second]
        val_2[part, me] = acc.astype(bf16)
        stat_2[part, me] = jnp.where(sub == 0, peak, jnp.where(sub == 1, weight_sum, anchor))
    stat_waits = [exchange(stat_2.at[part], ORDERS[part][1]) for part in range(2)]
    val_waits = [exchange(val_2.at[part], ORDERS[part][1]) for part in range(2)]

    wo_load.wait()
    attended, logs = [], []
    for part in range(2):
        arrived(stat_waits[part])
        arrived(val_waits[part])
        peak, weight_sum, anchor, acc = combined(
            part, val_2.at[part], stat_2.at[part], sizes[ORDERS[part][1]], True
        )
        attended.append(acc)
        logs.append(peak + jnp.log(weight_sum) + anchor)
    attended = jnp.concatenate(attended, axis=1).astype(bf16)
    part_out = jnp.dot(attended, wo_v[...], preferred_element_type=f32)
    out_x[place["tp"]] = part_out.astype(bf16)
    out_waits = exchange(out_x, "tp")

    logs = jnp.where(iota((8, 128), 1) < rows // 2, logs[0], logs[1]).T
    found = jnp.zeros((batch, heads), f32)
    for h in range(heads):
        found = jnp.where(iota((batch, heads), 1) == h, logs[h * batch : (h + 1) * batch, :1], found)
    log_weight[...] = found

    arrived(out_waits)
    mixed[...] = total(out_x, n_tp).astype(bf16)
    for out in sent:
        out.wait_send()


def shards(*args):
    (tokens, gain, w_query, w_key, w_value, gate_w, gate_bias, cache, cum, lengths, w_out) = args
    n_kv0, n_kv1, n_tp = (lax.axis_size(a) for a in ("kv_0", "kv_1", "tp"))
    batch, cols = tokens.shape
    span, head = cache.shape[1], cache.shape[3] // 2
    heads = cum.shape[1]
    rows = heads * batch
    half = batch // 2
    copies = 2 * (4 * 2 * (n_kv0 + n_kv1 - 2) // 2) + n_tp - 1
    anywhere = pl.BlockSpec(memory_space=pl.ANY)
    scalars = pl.BlockSpec(memory_space=pltpu.SMEM)
    n = max(n_kv0, n_kv1)
    in_specs = [anywhere] * 6 + [scalars] + [anywhere] * 2 + [scalars, anywhere]
    return pl.pallas_call(
        functools.partial(kernel, n_kv0, n_kv1, n_tp),
        out_shape=(
            jax.ShapeDtypeStruct((batch, w_out.shape[1]), bf16),
            jax.ShapeDtypeStruct((batch, heads), f32),
        ),
        in_specs=in_specs,
        out_specs=(pl.BlockSpec(memory_space=pltpu.VMEM), pl.BlockSpec(memory_space=pltpu.VMEM)),
        scratch_shapes=[
            pltpu.VMEM((batch, cols), bf16),
            pltpu.VMEM((1, cols), f32),
            pltpu.VMEM(w_query.shape, bf16),
            pltpu.VMEM((2 * head, cols), bf16),
            pltpu.VMEM((128, cols), bf16),
            pltpu.VMEM(w_out.shape, bf16),
            pltpu.VMEM((batch, span, 2 * head), bf16),
            pltpu.VMEM(cum.shape, f32),
            pltpu.VMEM((batch * head, span), bf16),
            pltpu.VMEM((rows, span), f32),
            pltpu.VMEM((rows, span), f32),
            pltpu.VMEM((rows, span), bf16),
            pltpu.VMEM((2, n, half, heads * head + 128), bf16),
            pltpu.VMEM((2, n, half, heads * head + 128), bf16),
            pltpu.VMEM((2, n, half, 128), bf16),
            pltpu.VMEM((2, n, half, 128), bf16),
            pltpu.VMEM((2, n, batch, 128), bf16),
            pltpu.VMEM((2, n, batch, 128), bf16),
            pltpu.VMEM((2, n, 8, 128), f32),
            pltpu.VMEM((2, n, 8, 128), f32),
            pltpu.VMEM((n_tp, batch, w_out.shape[1]), bf16),
            pltpu.SemaphoreType.DMA((16,)),
            pltpu.SemaphoreType.DMA((64,)),
            pltpu.SemaphoreType.DMA((64,)),
        ],
        compiler_params=pltpu.CompilerParams(
            collective_id=0, has_side_effects=True, vmem_limit_bytes=60 * 1024 * 1024
        ),
    )(
        tokens,
        gain.reshape(1, cols),
        w_query,
        w_key.T,
        w_value.T,
        gate_w.T,
        gate_bias,
        cache.reshape(batch, span, 2 * head),
        cum,
        lengths,
        w_out,
    )


def solution(mesh):
    torus = Mesh(mesh.devices.reshape(4, 4, mesh.shape["tp"]), ("kv_0", "kv_1", "tp"))
    placed = (
        P(None, KV),
        P(KV),
        P(KV, "tp"),
        P(KV, "tp"),
        P(KV, "tp"),
        P(),
        P("tp"),
        P(None, KV, "tp", None),
        P(None, "tp", KV),
        P(),
        P("tp", KV),
    )
    return jax.shard_map(
        shards, mesh=torus, in_specs=placed, out_specs=(P(None, KV), P(None, "tp")), check_vma=False
    )
```

```python
import functools
import itertools

import jax
import jax.numpy as jnp
from jax import lax
from jax.experimental import pallas as pl
from jax.experimental.pallas import tpu as pltpu
from jax.sharding import Mesh
from jax.sharding import PartitionSpec as P

KV = ("kv_0", "kv_1")
MESH = pl.DeviceIdType.MESH
NT = (((1,), (1,)), ((), ()))
norm_eps = 1e-05
masked_floor = -1e30
empty_peak = -1e29
f32, bf16 = jnp.float32, jnp.bfloat16


def iota(shape, axis):
    return lax.broadcasted_iota(jnp.int32, shape, axis)


def hops(offset, sizes):
    return sum(min(o, n - o) for o, n in zip(offset, sizes))


def kernel(
    n_kv0,
    n_kv1,
    n_tp,
    tokens,
    gain,
    w_query,
    w_key,
    w_value,
    gate_rows,
    gate_bias,
    cache,
    cum,
    lengths,
    w_out,
    mixed,
    log_weight,
    tok_v,
    gain_v,
    wq_v,
    wkv_v,
    wg_v,
    wo_v,
    bias_s,
    len_s,
    cache_v,
    cum_v,
    keys_t,
    cum_neg,
    biased,
    weights,
    query_x,
    gate_x,
    new_x,
    val_x,
    stat_x,
    out_x,
    load_sem,
    send_sem,
    recv_sem,
):
    at = tuple(lax.axis_index(a) for a in ("kv_0", "kv_1", "tp"))
    sizes = (n_kv0, n_kv1, n_tp)
    n_kv = n_kv0 * n_kv1
    kv_index = at[0] * n_kv1 + at[1]
    batch, span = cache.shape[0], cache.shape[1]
    cols = tokens.shape[1]
    heads = cum.shape[1]
    head = cache.shape[2] // 2
    rows = heads * batch
    half = batch // 2
    width = cols * n_kv
    n_gates = gate_rows.shape[0]

    count = itertools.count()

    def load(src, dst):
        copy = pltpu.make_async_copy(src, dst, load_sem.at[next(count)])
        copy.start()
        return copy

    mine = gate_rows.at[:, pl.ds(pl.multiple_of(kv_index * cols, cols), cols)]
    small = [
        load(tokens, tok_v),
        load(gain, gain_v),
        load(w_query, wq_v),
        load(mine, wg_v.at[pl.ds(0, n_gates)]),
        load(mine, wg_v.at[pl.ds(64, n_gates)]),
        load(w_key, wkv_v.at[pl.ds(0, head)]),
        load(w_value, wkv_v.at[pl.ds(head, head)]),
    ]

    kv_offsets = [(a, b, 0) for a in range(n_kv0) for b in range(n_kv1) if a or b]
    tp_offsets = [(0, 0, c) for c in range(1, n_tp)]
    kv_offsets.sort(key=lambda o: -hops(o, sizes))
    tp_offsets.sort(key=lambda o: -hops(o, sizes))

    def peer(offset, sign=1):
        return tuple(
            lax.rem(p + (o if sign > 0 else n - o), n) if o else p for p, o, n in zip(at, offset, sizes)
        )

    barrier = pltpu.get_barrier_semaphore()
    for offset in kv_offsets + tp_offsets:
        pl.semaphore_signal(barrier, inc=1, device_id=peer(offset), device_id_type=MESH)

    scalar_loads = [load(lengths, len_s), load(gate_bias, bias_s)]
    cum_load = load(cum, cum_v)
    block = batch // 8
    first_cache = next(count)
    for k in range(8):
        pltpu.make_async_copy(
            cache.at[pl.ds(k * block, block)],
            cache_v.at[pl.ds(k * block, block)],
            load_sem.at[first_cache + k],
        ).start()
    for k in range(7):
        next(count)
    wo_load = load(w_out, wo_v)

    numbers = itertools.count()
    sent = []

    def slot(place, offsets):
        return place[0] * n_kv1 + place[1] if offsets is kv_offsets else place[2]

    def exchange(buffer, offsets):
        waits = []
        for offset in offsets:
            number = next(numbers)
            there, source = peer(offset), peer(offset, -1)
            me, came = slot(at, offsets), slot(source, offsets)
            out = pltpu.make_async_remote_copy(
                src_ref=buffer.at[me],
                dst_ref=buffer.at[me],
                send_sem=send_sem.at[number],
                recv_sem=recv_sem.at[number],
                device_id=there,
                device_id_type=MESH,
            )
            out.start()
            sent.append(out)
            waits.append(
                (
                    came,
                    pltpu.make_async_remote_copy(
                        src_ref=buffer.at[came],
                        dst_ref=buffer.at[came],
                        send_sem=send_sem.at[number],
                        recv_sem=recv_sem.at[number],
                        device_id=source,
                        device_id_type=MESH,
                    ),
                )
            )
        return waits[::-1]

    wg_v[n_gates:64, :] = jnp.zeros((64 - n_gates, cols), bf16)
    wg_v[64 + n_gates :, :] = jnp.zeros((64 - n_gates, cols), bf16)
    for copy in small[:5]:
        copy.wait()
    tokens_f = tok_v[...].astype(f32)
    squares = jnp.sum(tokens_f * tokens_f, axis=1, keepdims=True)
    normed = (tokens_f * gain_v[...]).astype(bf16)
    lane = iota((batch, 128), 1)
    half_lane = iota((half, 128), 1)
    query_x[kv_index] = jnp.dot(normed, wq_v[...], preferred_element_type=f32).astype(bf16)
    part_gate = lax.dot_general(normed, wg_v[...], NT, preferred_element_type=f32)
    part_gate = jnp.where(lane % 64 < n_gates, part_gate, squares)
    gate_x[kv_index] = jnp.where(half_lane < 64, part_gate[:half], part_gate[half:]).astype(bf16)

    pl.semaphore_wait(barrier, len(kv_offsets) + len(tp_offsets))
    query_waits = exchange(query_x, kv_offsets)
    gate_waits = exchange(gate_x, kv_offsets)
    for copy in small[5:]:
        copy.wait()
    new_x[kv_index] = lax.dot_general(normed, wkv_v[...], NT, preferred_element_type=f32).astype(bf16)
    new_waits = exchange(new_x, kv_offsets)

    for copy in scalar_loads:
        copy.wait()
    cum_load.wait()
    first_pos = kv_index * span
    length_rows = jnp.zeros((batch, 128), jnp.int32)
    for b in range(batch):
        length_rows = jnp.where(iota((batch, 128), 0) == b, len_s[b], length_rows)
    length_col = length_rows[:, :1] - first_pos
    last_parts = []
    for h in range(heads):
        last = jnp.zeros((batch, 128), f32)
        for n in range(span // 128):
            position = iota((batch, 128), 1) + n * 128
            value = cum_v[:, h, n * 128 : (n + 1) * 128]
            cum_neg[h * batch : (h + 1) * batch, n * 128 : (n + 1) * 128] = jnp.where(
                position < length_col, -value, masked_floor
            )
            last = last + jnp.where(position == length_col - 1, value, 0.0)
        last_parts.append(jnp.sum(last, axis=1, keepdims=True))
    last_cum = jnp.concatenate(last_parts, axis=0)
    holds = (length_col > 0) & (length_col <= span)
    holds = jnp.concatenate([jnp.where(holds, 1, 0)] * heads, axis=0) > 0

    def flip(k, carry):
        pltpu.make_async_copy(
            cache.at[pl.ds(k * block, block)],
            cache_v.at[pl.ds(k * block, block)],
            load_sem.at[first_cache + k],
        ).wait()
        for j in range(block):
            b = k * block + j
            keys_t[pl.ds(pl.multiple_of(b * head, head), head), :] = cache_v[b].T[:head]
        return carry

    lax.fori_loop(0, 8, flip, 0)

    sum_query = query_x[kv_index].astype(f32)
    for came, wait in query_waits:
        wait.wait_recv()
        sum_query = sum_query + query_x[came].astype(f32)
    gates = gate_x[kv_index].astype(f32)
    for came, wait in gate_waits:
        wait.wait_recv()
        gates = gates + gate_x[came].astype(f32)
    total_squares = jnp.concatenate(
        [gates[:, n_gates : n_gates + 1], gates[:, 64 + n_gates : 65 + n_gates]], axis=0
    )
    row_scale = lax.rsqrt(total_squares / width + norm_eps)
    query = (row_scale * sum_query).astype(bf16).astype(f32)
    log_gate = []
    for h in range(heads):
        pick = at[2] * heads + h
        logit = jnp.concatenate(
            [
                jnp.sum(jnp.where(half_lane == pick + 64 * part, gates, 0.0), axis=1, keepdims=True)
                for part in range(2)
            ],
            axis=0,
        )
        logit = row_scale * logit + bias_s[h]
        log_gate.append(jnp.minimum(logit, 0.0) - jnp.log1p(jnp.exp(-jnp.abs(logit))))
    cum_query = last_cum + jnp.concatenate(log_gate, axis=0)

    doubled = []
    for pair in range(heads // 2):
        two = query[:, pair * 128 : (pair + 1) * 128]
        turned = pltpu.roll(two, 64, 1)
        doubled.append(jnp.where(lane < head, two, turned))
        doubled.append(jnp.where(lane < head, turned, two))
    doubled = jnp.concatenate(doubled, axis=0)
    row_of = iota((rows, 128), 0) % batch
    lane_of = iota((rows, 128), 1)
    side = jnp.where(lane_of < head, 0, 1)
    inv_root = head ** (-0.5)
    scaled = doubled * inv_root
    spread = jnp.concatenate(
        [jnp.where(row_of == 2 * p + side, scaled, 0.0).astype(bf16) for p in range(batch // 2)], axis=1
    )

    tile = 256
    peak = jnp.full((rows, 128), masked_floor, f32)
    for n in range(span // tile):
        cut = slice(n * tile, (n + 1) * tile)
        score = jnp.dot(spread, keys_t[:, cut], preferred_element_type=f32) + cum_neg[:, cut]
        biased[:, cut] = score
        for k in range(tile // 128):
            peak = jnp.maximum(peak, score[:, k * 128 : (k + 1) * 128])

    new_rows = new_x[kv_index].astype(f32)
    for came, wait in new_waits:
        wait.wait_recv()
        new_rows = new_rows + new_x[came].astype(f32)
    new_rows = (row_scale * new_rows).astype(bf16).astype(f32)
    new_rows = jnp.concatenate([new_rows] * heads, axis=0)
    new_biased = (
        jnp.sum(jnp.where(lane_of < head, doubled * new_rows, 0.0), axis=1, keepdims=True) * inv_root
        - cum_query
    )

    peak = jnp.max(peak, axis=1, keepdims=True)
    peak = jnp.where(holds, jnp.maximum(peak, new_biased), peak)
    peak = jnp.maximum(peak, empty_peak)
    sums = jnp.zeros((rows, 128), f32)
    for n in range(span // 128):
        cut = slice(n * 128, (n + 1) * 128)
        weight = jnp.exp(biased[:, cut] - peak)
        sums = sums + weight
        weights[:, cut] = weight.astype(bf16)
    new_weight = jnp.where(holds, jnp.exp(new_biased - peak), 0.0)
    weight_sum = jnp.sum(sums, axis=1, keepdims=True) + new_weight

    diagonal = iota((rows, 128), 0) == lane_of

    def as_row(column):
        return jnp.sum(jnp.where(diagonal, column, 0.0), axis=0, keepdims=True)

    sub = iota((8, 128), 0)
    anchor = jnp.where(holds, cum_query, 0.0)
    stat_x[kv_index] = jnp.where(
        sub == 0, as_row(peak), jnp.where(sub == 1, as_row(weight_sum), as_row(anchor))
    )
    stat_waits = exchange(stat_x, kv_offsets)

    values = new_weight.astype(bf16).astype(f32) * new_rows
    for p in range(batch // 2):
        both = jnp.concatenate([cache_v[2 * p], cache_v[2 * p + 1]], axis=1)
        out = jnp.dot(weights[...], both, preferred_element_type=f32)
        values = (
            values
            + jnp.where(row_of == 2 * p, out[:, :128], 0.0)
            + jnp.where(row_of == 2 * p + 1, out[:, 128:], 0.0)
        )
    val_x[kv_index] = values.T[head:].astype(bf16)
    val_waits = exchange(val_x, kv_offsets)

    wo_load.wait()
    for _, wait in stat_waits:
        wait.wait_recv()
    peaks = stat_x[:, 0, :]
    peak = jnp.max(peaks, axis=0, keepdims=True)
    factors = jnp.exp(peaks - peak)
    weight_sum = jnp.sum(stat_x[:, 1, :] * factors, axis=0, keepdims=True)
    logs = peak + jnp.log(weight_sum) + jnp.sum(stat_x[:, 2, :], axis=0, keepdims=True)
    factors = factors / weight_sum
    log_weight[...] = jnp.concatenate([logs[:, h * batch : (h + 1) * batch] for h in range(heads)], axis=0)
    for _, wait in val_waits:
        wait.wait_recv()
    acc = val_x[0].astype(f32) * factors[0:1]
    for k in range(1, n_kv):
        acc = acc + val_x[k].astype(f32) * factors[k : k + 1]
    attended = acc.T.astype(bf16)
    part_out = jnp.zeros((batch, w_out.shape[1]), f32)
    for h in range(heads):
        part_out = part_out + jnp.dot(
            attended[h * batch : (h + 1) * batch],
            wo_v[h * head : (h + 1) * head],
            preferred_element_type=f32,
        )
    out_x[at[2]] = part_out.astype(bf16)
    out_waits = exchange(out_x, tp_offsets)
    for _, wait in out_waits:
        wait.wait_recv()
    acc = out_x[0].astype(f32)
    for k in range(1, n_tp):
        acc = acc + out_x[k].astype(f32)
    mixed[...] = acc.astype(bf16)
    for out in sent:
        out.wait_send()


def shards(*args):
    (tokens, gain, w_query, w_key, w_value, gate_w, gate_bias, cache, cum, lengths, w_out) = args
    n_kv0, n_kv1, n_tp = (lax.axis_size(a) for a in ("kv_0", "kv_1", "tp"))
    n_kv = n_kv0 * n_kv1
    batch, cols = tokens.shape
    span, head = cache.shape[1], cache.shape[3] // 2
    heads = cum.shape[1]
    rows = heads * batch
    half = batch // 2
    copies = 5 * (n_kv - 1) + n_tp - 1
    anywhere = pl.BlockSpec(memory_space=pl.ANY)
    near = pl.BlockSpec(memory_space=pltpu.VMEM)
    mixed, logs = pl.pallas_call(
        functools.partial(kernel, n_kv0, n_kv1, n_tp),
        out_shape=(
            pltpu.VMEM((batch, w_out.shape[1]), bf16),
            pltpu.VMEM((heads, batch), f32),
        ),
        in_specs=[anywhere] * len(args),
        out_specs=(near, near),
        scratch_shapes=[
            pltpu.VMEM((batch, cols), bf16),
            pltpu.VMEM((1, cols), f32),
            pltpu.VMEM(w_query.shape, bf16),
            pltpu.VMEM((2 * head, cols), bf16),
            pltpu.VMEM((128, cols), bf16),
            pltpu.VMEM(w_out.shape, bf16),
            pltpu.SMEM(gate_bias.shape, f32),
            pltpu.SMEM(lengths.shape, jnp.int32),
            pltpu.VMEM((batch, span, 2 * head), bf16),
            pltpu.VMEM(cum.shape, f32),
            pltpu.VMEM((batch * head, span), bf16),
            pltpu.VMEM((rows, span), f32),
            pltpu.VMEM((rows, span), f32),
            pltpu.VMEM((rows, span), bf16),
            pltpu.VMEM((n_kv, batch, heads * head), bf16),
            pltpu.VMEM((n_kv, half, 128), bf16),
            pltpu.VMEM((n_kv, batch, 2 * head), bf16),
            pltpu.VMEM((n_kv, head, rows), bf16),
            pltpu.VMEM((n_kv, 8, rows), f32),
            pltpu.VMEM((n_tp, batch, w_out.shape[1]), bf16),
            pltpu.SemaphoreType.DMA((24,)),
            pltpu.SemaphoreType.DMA((copies,)),
            pltpu.SemaphoreType.DMA((copies,)),
        ],
        compiler_params=pltpu.CompilerParams(
            collective_id=0, has_side_effects=True, vmem_limit_bytes=60 * 1024 * 1024
        ),
    )(
        tokens,
        gain.reshape(1, cols),
        w_query,
        w_key.T,
        w_value.T,
        gate_w.T,
        gate_bias,
        cache.reshape(batch, span, 2 * head),
        cum,
        lengths,
        w_out,
    )
    return mixed, logs.T


def solution(mesh):
    torus = Mesh(mesh.devices.reshape(4, 4, mesh.shape["tp"]), ("kv_0", "kv_1", "tp"))
    placed = (
        P(None, KV),
        P(KV),
        P(KV, "tp"),
        P(KV, "tp"),
        P(KV, "tp"),
        P(),
        P("tp"),
        P(None, KV, "tp", None),
        P(None, "tp", KV),
        P(),
        P("tp", KV),
    )
    return jax.shard_map(
        shards, mesh=torus, in_specs=placed, out_specs=(P(None, KV), P(None, "tp")), check_vma=False
    )
```

```python
import functools
import itertools

import jax
import jax.numpy as jnp
from jax import lax
from jax.experimental import pallas as pl
from jax.experimental.pallas import tpu as pltpu
from jax.sharding import Mesh
from jax.sharding import PartitionSpec as P

KV = ("kv_0", "kv_1")
MESH = pl.DeviceIdType.MESH
NT = (((1,), (1,)), ((), ()))
norm_eps = 1e-05
masked_floor = -1e30
empty_peak = -1e29
f32, bf16 = jnp.float32, jnp.bfloat16


def iota(shape, axis):
    return lax.broadcasted_iota(jnp.int32, shape, axis)


def hops(offset, sizes):
    return sum(min(o, n - o) for o, n in zip(offset, sizes))


def kernel(
    n_kv0,
    n_kv1,
    n_tp,
    tokens,
    gain,
    w_query,
    w_key,
    w_value,
    gate_rows,
    gate_bias,
    cache,
    cum,
    lengths,
    w_out,
    mixed,
    log_weight,
    tok_v,
    gain_v,
    wq_v,
    wkv_v,
    wg_v,
    wo_v,
    bias_s,
    len_s,
    cache_v,
    cum_v,
    keys_t,
    packed,
    cum_neg,
    biased,
    weights,
    query_x,
    new_x,
    val_x,
    stat_x,
    out_x,
    load_sem,
    send_sem,
    recv_sem,
):
    at = tuple(lax.axis_index(a) for a in ("kv_0", "kv_1", "tp"))
    sizes = (n_kv0, n_kv1, n_tp)
    n_kv = n_kv0 * n_kv1
    kv_index = at[0] * n_kv1 + at[1]
    batch, span = cache.shape[0], cache.shape[1]
    cols = tokens.shape[1]
    heads = cum.shape[1]
    head = cache.shape[2] // 2
    rows = heads * batch
    width = cols * n_kv
    n_gates = gate_rows.shape[0]

    def load(number, src, dst):
        copy = pltpu.make_async_copy(src, dst, load_sem.at[number])
        copy.start()
        return copy

    mine = gate_rows.at[:, pl.ds(pl.multiple_of(kv_index * cols, cols), cols)]
    small = [load(0, tokens, tok_v), load(0, gain, gain_v), load(0, w_query, wq_v)]
    small += [load(0, mine, wg_v.at[pl.ds(64 * k, n_gates)]) for k in range(4)]
    small_new = [load(1, w_key, wkv_v.at[pl.ds(0, head)]), load(1, w_value, wkv_v.at[pl.ds(head, head)])]

    kv_offsets = [(a, b, 0) for a in range(n_kv0) for b in range(n_kv1) if a or b]
    tp_offsets = [(0, 0, c) for c in range(1, n_tp)]
    kv_offsets.sort(key=lambda o: -hops(o, sizes))
    tp_offsets.sort(key=lambda o: -hops(o, sizes))

    def moved(p, o, n):
        return jnp.where(p + o >= n, p + o - n, p + o) if o else p

    def peer(offset, sign=1):
        return tuple(moved(p, o if sign > 0 else (n - o) % n, n) for p, o, n in zip(at, offset, sizes))

    barrier = pltpu.get_barrier_semaphore()
    for offset in kv_offsets + tp_offsets:
        pl.semaphore_signal(barrier, inc=1, device_id=peer(offset), device_id_type=MESH)

    scalar_loads = [load(2, lengths, len_s), load(2, gate_bias, bias_s)]
    cum_load = load(3, cum, cum_v)
    blocks = 4
    block = batch // blocks

    def cache_copy(k):
        part = pl.ds(k * block, block)
        return pltpu.make_async_copy(cache.at[part], cache_v.at[part], load_sem.at[5 + k])

    for k in range(blocks):
        cache_copy(k).start()
    wo_load = load(4, w_out, wo_v)

    numbers = itertools.count()
    sent = []

    def exchange(buffer, offsets):
        number = next(numbers)
        me = kv_index if offsets is kv_offsets else at[2]
        for offset in offsets:
            pltpu.make_async_remote_copy(
                src_ref=buffer.at[me],
                dst_ref=buffer.at[me],
                send_sem=send_sem.at[number],
                recv_sem=recv_sem.at[number],
                device_id=peer(offset),
                device_id_type=MESH,
            ).start()
        others = buffer.at[pl.ds(0, len(offsets))]
        every = pltpu.make_async_remote_copy(
            src_ref=others,
            dst_ref=others,
            send_sem=send_sem.at[number],
            recv_sem=recv_sem.at[number],
            device_id=peer(offsets[0]),
            device_id_type=MESH,
        )
        sent.append(every)
        return every

    for k in range(4):
        wg_v[64 * k + n_gates : 64 * (k + 1), :] = jnp.zeros((64 - n_gates, cols), bf16)
    for copy in small:
        copy.wait()
    tokens_f = tok_v[...].astype(f32)
    squares = jnp.sum(tokens_f * tokens_f, axis=1, keepdims=True)
    normed = (tokens_f * gain_v[...]).astype(bf16)
    lane = iota((batch, 128), 1)
    fold = batch // 4
    fold_lane = iota((fold, 256), 1)
    query_x[kv_index, :batch] = jnp.dot(normed, wq_v[...], preferred_element_type=f32).astype(bf16)
    part_gate = lax.dot_general(normed, wg_v[...], NT, preferred_element_type=f32)
    part_gate = jnp.where(iota((batch, 256), 1) % 64 < n_gates, part_gate, squares)
    folded = part_gate[:fold]
    for k in range(1, 4):
        folded = jnp.where(fold_lane >= 64 * k, part_gate[k * fold : (k + 1) * fold], folded)
    query_x[kv_index, batch:] = folded.astype(bf16)

    pl.semaphore_wait(barrier, len(kv_offsets) + len(tp_offsets))
    query_all = exchange(query_x, kv_offsets)
    for copy in small_new:
        copy.wait()
    new_x[kv_index] = lax.dot_general(normed, wkv_v[...], NT, preferred_element_type=f32).astype(bf16)
    new_all = exchange(new_x, kv_offsets)

    for copy in scalar_loads:
        copy.wait()
    cum_load.wait()
    first_pos = kv_index * span
    length_rows = jnp.zeros((batch, 128), jnp.int32)
    for b in range(batch):
        length_rows = jnp.where(iota((batch, 128), 0) == b, len_s[b], length_rows)
    length_col = length_rows[:, :1] - first_pos
    last_parts = []
    for h in range(heads):
        last = jnp.zeros((batch, 128), f32)
        for n in range(span // 128):
            position = iota((batch, 128), 1) + n * 128
            value = cum_v[:, h, n * 128 : (n + 1) * 128]
            cum_neg[h * batch : (h + 1) * batch, n * 128 : (n + 1) * 128] = jnp.where(
                position < length_col, -value, masked_floor
            )
            last = last + jnp.where(position == length_col - 1, value, 0.0)
        last_parts.append(jnp.sum(last, axis=1, keepdims=True))
    last_cum = jnp.concatenate(last_parts, axis=0)
    holds = (length_col > 0) & (length_col <= span)
    holds = jnp.concatenate([jnp.where(holds, 1, 0)] * heads, axis=0) > 0

    column = iota((4 * head, 2 * head), 1)
    chosen = jnp.where(column < head, column + head, column + 2 * head)
    chooser = jnp.where(iota((4 * head, 2 * head), 0) == chosen, 1.0, 0.0).astype(bf16)
    for k in range(blocks):
        cache_copy(k).wait()

        def prepare(j, carry, k=k):
            b = 2 * (k * block // 2 + j)
            pair = jnp.concatenate([cache_v[b], cache_v[b + 1]], axis=1)
            packed[k * block // 2 + j] = jnp.dot(pair, chooser, preferred_element_type=f32).astype(bf16)
            for i in range(2):
                keys_t[pl.ds(pl.multiple_of((b + i) * head, head), head), :] = cache_v[b + i].T[:head]
            return carry

        lax.fori_loop(0, block // 2, prepare, 0)

    query_all.wait_recv()
    total = query_x[0].astype(f32)
    for k in range(1, n_kv):
        total = total + query_x[k].astype(f32)
    sum_query, gates = total[:batch], total[batch:]
    total_squares = jnp.concatenate(
        [gates[:, 64 * k + n_gates : 64 * k + n_gates + 1] for k in range(4)], axis=0
    )
    row_scale = lax.rsqrt(total_squares / width + norm_eps)
    query = (row_scale * sum_query).astype(bf16).astype(f32)
    log_gate = []
    for h in range(heads):
        pick = at[2] * heads + h
        logit = jnp.concatenate(
            [
                jnp.sum(jnp.where(fold_lane == pick + 64 * k, gates, 0.0), axis=1, keepdims=True)
                for k in range(4)
            ],
            axis=0,
        )
        logit = row_scale * logit + bias_s[h]
        log_gate.append(jnp.minimum(logit, 0.0) - jnp.log1p(jnp.exp(-jnp.abs(logit))))
    cum_query = last_cum + jnp.concatenate(log_gate, axis=0)

    doubled = []
    for pair in range(heads // 2):
        two = query[:, pair * 128 : (pair + 1) * 128]
        turned = pltpu.roll(two, 64, 1)
        doubled.append(jnp.where(lane < head, two, turned))
        doubled.append(jnp.where(lane < head, turned, two))
    doubled = jnp.concatenate(doubled, axis=0)
    row_of = iota((rows, 128), 0) % batch
    lane_of = iota((rows, 128), 1)
    side = jnp.where(lane_of < head, 0, 1)
    inv_root = head ** (-0.5)
    scaled = doubled * inv_root
    spread = jnp.concatenate(
        [jnp.where(row_of == 2 * p + side, scaled, 0.0).astype(bf16) for p in range(batch // 2)], axis=1
    )

    tile = 256
    peak = jnp.full((rows, 128), masked_floor, f32)
    for n in range(span // tile):
        cut = slice(n * tile, (n + 1) * tile)
        score = jnp.dot(spread, keys_t[:, cut], preferred_element_type=f32) + cum_neg[:, cut]
        biased[:, cut] = score
        for k in range(tile // 128):
            peak = jnp.maximum(peak, score[:, k * 128 : (k + 1) * 128])

    new_all.wait_recv()
    new_rows = new_x[0].astype(f32)
    for k in range(1, n_kv):
        new_rows = new_rows + new_x[k].astype(f32)
    new_rows = (row_scale * new_rows).astype(bf16).astype(f32)
    new_rows = jnp.concatenate([new_rows] * heads, axis=0)
    new_biased = (
        jnp.sum(jnp.where(lane_of < head, doubled * new_rows, 0.0), axis=1, keepdims=True) * inv_root
        - cum_query
    )

    peak = jnp.max(peak, axis=1, keepdims=True)
    peak = jnp.where(holds, jnp.maximum(peak, new_biased), peak)
    peak = jnp.maximum(peak, empty_peak)
    sums = jnp.zeros((rows, 128), f32)
    for n in range(span // 128):
        cut = slice(n * 128, (n + 1) * 128)
        weight = jnp.exp(biased[:, cut] - peak)
        sums = sums + weight
        weights[:, cut] = weight.astype(bf16)
    new_weight = jnp.where(holds, jnp.exp(new_biased - peak), 0.0)
    weight_sum = jnp.sum(sums, axis=1, keepdims=True) + new_weight

    diagonal = iota((rows, 128), 0) == lane_of

    def as_row(column):
        return jnp.sum(jnp.where(diagonal, column, 0.0), axis=0, keepdims=True)

    sub = iota((8, 128), 0)
    anchor = jnp.where(holds, cum_query, 0.0)
    stat_x[kv_index] = jnp.where(
        sub == 0, as_row(peak), jnp.where(sub == 1, as_row(weight_sum), as_row(anchor))
    )
    stat_all = exchange(stat_x, kv_offsets)

    values = jnp.where(lane_of < head, 0.0, new_weight.astype(bf16).astype(f32) * new_rows)
    for q in range(batch // 4):
        four = jnp.concatenate([packed[2 * q], packed[2 * q + 1]], axis=1)
        out = jnp.dot(weights[...], four, preferred_element_type=f32)
        for i in range(2):
            values = values + jnp.where(row_of == 4 * q + 2 * i + side, out[:, 128 * i : 128 * (i + 1)], 0.0)
    turned = values.T
    val_x[kv_index] = (turned[:head] + turned[head:]).astype(bf16)
    val_all = exchange(val_x, kv_offsets)

    wo_load.wait()
    stat_all.wait_recv()
    peaks = stat_x[:, 0, :]
    peak = jnp.max(peaks, axis=0, keepdims=True)
    factors = jnp.exp(peaks - peak)
    weight_sum = jnp.sum(stat_x[:, 1, :] * factors, axis=0, keepdims=True)
    logs = peak + jnp.log(weight_sum) + jnp.sum(stat_x[:, 2, :], axis=0, keepdims=True)
    factors = factors / weight_sum
    log_weight[...] = jnp.concatenate([logs[:, h * batch : (h + 1) * batch] for h in range(heads)], axis=0)
    val_all.wait_recv()
    acc = val_x[0].astype(f32) * factors[0:1]
    for k in range(1, n_kv):
        acc = acc + val_x[k].astype(f32) * factors[k : k + 1]
    attended = acc.T.astype(bf16)
    part_out = jnp.zeros((batch, w_out.shape[1]), f32)
    for h in range(heads):
        part_out = part_out + jnp.dot(
            attended[h * batch : (h + 1) * batch],
            wo_v[h * head : (h + 1) * head],
            preferred_element_type=f32,
        )
    out_x[at[2]] = part_out.astype(bf16)
    exchange(out_x, tp_offsets).wait_recv()
    acc = out_x[0].astype(f32)
    for k in range(1, n_tp):
        acc = acc + out_x[k].astype(f32)
    mixed[...] = acc.astype(bf16)
    for every in sent:
        every.wait_send()


def store(mixed, log_weight, mixed_out, log_out, sem):
    copies = [
        pltpu.make_async_copy(mixed, mixed_out, sem.at[0]),
        pltpu.make_async_copy(log_weight, log_out, sem.at[1]),
    ]
    for copy in copies:
        copy.start()
    for copy in copies:
        copy.wait()


def shards(*args):
    (tokens, gain, w_query, w_key, w_value, gate_w, gate_bias, cache, cum, lengths, w_out) = args
    n_kv0, n_kv1, n_tp = (lax.axis_size(a) for a in ("kv_0", "kv_1", "tp"))
    n_kv = n_kv0 * n_kv1
    batch, cols = tokens.shape
    span, head = cache.shape[1], cache.shape[3] // 2
    heads = cum.shape[1]
    rows = heads * batch
    anywhere = pl.BlockSpec(memory_space=pl.ANY)
    near = pl.BlockSpec(memory_space=pltpu.VMEM)
    mixed, logs = pl.pallas_call(
        functools.partial(kernel, n_kv0, n_kv1, n_tp),
        out_shape=(
            pltpu.VMEM((batch, w_out.shape[1]), bf16),
            pltpu.VMEM((heads, batch), f32),
        ),
        in_specs=[anywhere] * len(args),
        out_specs=(near, near),
        scratch_shapes=[
            pltpu.VMEM((batch, cols), bf16),
            pltpu.VMEM((1, cols), f32),
            pltpu.VMEM(w_query.shape, bf16),
            pltpu.VMEM((2 * head, cols), bf16),
            pltpu.VMEM((256, cols), bf16),
            pltpu.VMEM(w_out.shape, bf16),
            pltpu.SMEM(gate_bias.shape, f32),
            pltpu.SMEM(lengths.shape, jnp.int32),
            pltpu.VMEM((batch, span, 2 * head), bf16),
            pltpu.VMEM(cum.shape, f32),
            pltpu.VMEM((batch * head, span), bf16),
            pltpu.VMEM((batch // 2, span, 2 * head), bf16),
            pltpu.VMEM((rows, span), f32),
            pltpu.VMEM((rows, span), f32),
            pltpu.VMEM((rows, span), bf16),
            pltpu.VMEM((n_kv, batch + batch // 4, heads * head), bf16),
            pltpu.VMEM((n_kv, batch, 2 * head), bf16),
            pltpu.VMEM((n_kv, head, rows), bf16),
            pltpu.VMEM((n_kv, 8, rows), f32),
            pltpu.VMEM((n_tp, batch, w_out.shape[1]), bf16),
            pltpu.SemaphoreType.DMA((9,)),
            pltpu.SemaphoreType.DMA((5,)),
            pltpu.SemaphoreType.DMA((5,)),
        ],
        compiler_params=pltpu.CompilerParams(
            collective_id=0, has_side_effects=True, vmem_limit_bytes=60 * 1024 * 1024
        ),
    )(
        tokens,
        gain.reshape(1, cols),
        w_query,
        w_key.T,
        w_value.T,
        gate_w.T,
        gate_bias,
        cache.reshape(batch, span, 2 * head),
        cum,
        lengths,
        w_out,
    )
    mixed, logs = pl.pallas_call(
        store,
        out_shape=(jax.ShapeDtypeStruct(mixed.shape, bf16), jax.ShapeDtypeStruct(logs.shape, f32)),
        in_specs=(near, near),
        out_specs=(anywhere, anywhere),
        scratch_shapes=[pltpu.SemaphoreType.DMA((2,))],
        compiler_params=pltpu.CompilerParams(vmem_limit_bytes=1024 * 1024),
    )(mixed, logs)
    return mixed, logs.T


def solution(mesh):
    torus = Mesh(mesh.devices.reshape(4, 4, mesh.shape["tp"]), ("kv_0", "kv_1", "tp"))
    placed = (
        P(None, KV),
        P(KV),
        P(KV, "tp"),
        P(KV, "tp"),
        P(KV, "tp"),
        P(),
        P("tp"),
        P(None, KV, "tp", None),
        P(None, "tp", KV),
        P(),
        P("tp", KV),
    )
    return jax.shard_map(
        shards, mesh=torus, in_specs=placed, out_specs=(P(None, KV), P(None, "tp")), check_vma=False
    )
```

```python
import functools
import itertools

import jax
import jax.numpy as jnp
from jax import lax
from jax.experimental import pallas as pl
from jax.experimental.pallas import tpu as pltpu
from jax.sharding import Mesh
from jax.sharding import PartitionSpec as P

KV = ("kv_0", "kv_1")
MESH = pl.DeviceIdType.MESH
NT = (((1,), (1,)), ((), ()))
norm_eps = 1e-05
masked_floor = -1e30
empty_peak = -1e29
EARLY = 1
f32, bf16 = jnp.float32, jnp.bfloat16


def iota(shape, axis):
    return lax.broadcasted_iota(jnp.int32, shape, axis)


def hops(offset, sizes):
    return sum(min(o, n - o) for o, n in zip(offset, sizes))


def kernel(
    n_kv0,
    n_kv1,
    n_tp,
    tokens,
    gain,
    w_query,
    w_key,
    w_value,
    gate_rows,
    gate_bias,
    cache,
    cum,
    lengths,
    w_out,
    mixed,
    log_weight,
    tok_v,
    gain_v,
    wq_v,
    wkv_v,
    wg_v,
    wo_v,
    bias_s,
    len_s,
    cache_v,
    cum_v,
    keys_t,
    packed,
    cum_neg,
    biased,
    weights,
    query_1,
    query_2,
    new_1,
    new_2,
    val_x,
    stat_x,
    out_x,
    load_sem,
    send_sem,
    recv_sem,
):
    at = tuple(lax.axis_index(a) for a in ("kv_0", "kv_1", "tp"))
    sizes = (n_kv0, n_kv1, n_tp)
    n_kv = n_kv0 * n_kv1
    kv_index = at[0] * n_kv1 + at[1]
    batch, span = cache.shape[0], cache.shape[1]
    cols = tokens.shape[1]
    heads = cum.shape[1]
    head = cache.shape[2] // 2
    rows = heads * batch
    width = cols * n_kv
    n_gates = gate_rows.shape[0]

    def load(number, src, dst):
        copy = pltpu.make_async_copy(src, dst, load_sem.at[number])
        copy.start()
        return copy

    kv_offsets = [(a, b, 0) for a in range(n_kv0) for b in range(n_kv1) if a or b]
    tp_offsets = [(0, 0, c) for c in range(1, n_tp)]
    axis_offsets = ([(a, 0, 0) for a in range(1, n_kv0)], [(0, b, 0) for b in range(1, n_kv1)])
    for offsets in (kv_offsets, tp_offsets, *axis_offsets):
        offsets.sort(key=lambda o: (-hops(o, sizes), -sum(1 for c in o if c)))

    def moved(p, o, n):
        return jnp.where(p + o >= n, p + o - n, p + o) if o else p

    def peer(offset, sign=1):
        return tuple(moved(p, o if sign > 0 else (n - o) % n, n) for p, o, n in zip(at, offset, sizes))

    barrier = pltpu.get_barrier_semaphore()
    near_offsets = axis_offsets[0] + axis_offsets[1] + tp_offsets
    for offset in near_offsets:
        pl.semaphore_signal(barrier, inc=1, device_id=peer(offset), device_id_type=MESH)

    mine = gate_rows.at[:, pl.ds(pl.multiple_of(kv_index * cols, cols), cols)]
    small = [load(0, tokens, tok_v), load(0, gain, gain_v), load(0, w_query, wq_v)]
    small += [load(0, mine, wg_v.at[pl.ds(0, n_gates)])]
    small_new = [load(1, w_key, wkv_v.at[pl.ds(0, head)]), load(1, w_value, wkv_v.at[pl.ds(head, head)])]

    scalar_loads = [load(2, lengths, len_s), load(2, gate_bias, bias_s)]
    cum_load = load(3, cum, cum_v)
    blocks = 4
    block = batch // blocks

    def cache_copy(k):
        part = pl.ds(k * block, block)
        return pltpu.make_async_copy(cache.at[part], cache_v.at[part], load_sem.at[5 + k])

    for k in range(blocks):
        cache_copy(k).start()
    wo_load = load(4, w_out, wo_v)

    numbers = itertools.count()
    sent = []

    def exchange(buffer, *ways):
        number = next(numbers)
        copies = 0
        for me, offsets in ways:
            for offset in offsets:
                copies += 1
                pltpu.make_async_remote_copy(
                    src_ref=buffer.at[me],
                    dst_ref=buffer.at[me],
                    send_sem=send_sem.at[number],
                    recv_sem=recv_sem.at[number],
                    device_id=peer(offset),
                    device_id_type=MESH,
                ).start()
        others = buffer.at[pl.ds(0, copies)]
        every = pltpu.make_async_remote_copy(
            src_ref=others,
            dst_ref=others,
            send_sem=send_sem.at[number],
            recv_sem=recv_sem.at[number],
            device_id=peer(ways[0][1][0]),
            device_id_type=MESH,
        )
        sent.append(every)
        return every

    first_slots = (at[1], n_kv1 + at[0])
    first_ways = tuple(zip(first_slots, (axis_offsets[1], axis_offsets[0])))
    second_slots = (at[0], n_kv0 + at[1])
    second_ways = tuple(zip(second_slots, axis_offsets))

    def total(buffer, low, high):
        acc = buffer[low].astype(f32)
        for k in range(low + 1, high):
            acc = acc + buffer[k].astype(f32)
        return acc

    wg_v[n_gates:, :] = jnp.zeros((wg_v.shape[0] - n_gates, cols), bf16)
    for copy in small:
        copy.wait()
    tokens_f = tok_v[...].astype(f32)
    squares = jnp.sum(tokens_f * tokens_f, axis=1, keepdims=True)
    normed = (tokens_f * gain_v[...]).astype(bf16)
    lane = iota((batch, 128), 1)
    half = batch // 2
    part_query = jnp.dot(normed, wq_v[...], preferred_element_type=f32).astype(bf16)
    part_gate = lax.dot_general(normed, wg_v[...], NT, preferred_element_type=f32)
    part_gate = jnp.where(lane < n_gates, part_gate, squares).astype(bf16)
    for part in range(2):
        chunk = slice(part * half, (part + 1) * half)
        query_1[first_slots[part], :, : heads * head] = part_query[chunk]
        query_1[first_slots[part], :, heads * head :] = part_gate[chunk]

    pl.semaphore_wait(barrier, len(near_offsets))
    query_all = exchange(query_1, *first_ways)
    for copy in small_new:
        copy.wait()
    part_new = lax.dot_general(normed, wkv_v[...], NT, preferred_element_type=f32).astype(bf16)
    for part in range(2):
        new_1[first_slots[part]] = part_new[part * half : (part + 1) * half]
    new_all = exchange(new_1, *first_ways)

    for copy in scalar_loads:
        copy.wait()
    cum_load.wait()
    first_pos = kv_index * span
    length_rows = jnp.zeros((batch, 128), jnp.int32)
    for b in range(batch):
        length_rows = jnp.where(iota((batch, 128), 0) == b, len_s[b], length_rows)
    length_col = length_rows[:, :1] - first_pos
    last_parts = []
    for h in range(heads):
        last = jnp.zeros((batch, 128), f32)
        for n in range(span // 128):
            position = iota((batch, 128), 1) + n * 128
            value = cum_v[:, h, n * 128 : (n + 1) * 128]
            cum_neg[h * batch : (h + 1) * batch, n * 128 : (n + 1) * 128] = jnp.where(
                position < length_col, -value, masked_floor
            )
            last = last + jnp.where(position == length_col - 1, value, 0.0)
        last_parts.append(jnp.sum(last, axis=1, keepdims=True))
    last_cum = jnp.concatenate(last_parts, axis=0)
    holds = (length_col > 0) & (length_col <= span)
    holds = jnp.concatenate([jnp.where(holds, 1, 0)] * heads, axis=0) > 0

    column = iota((4 * head, 2 * head), 1)
    chosen = jnp.where(column < head, column + head, column + 2 * head)
    chooser = jnp.where(iota((4 * head, 2 * head), 0) == chosen, 1.0, 0.0).astype(bf16)

    def prepare(k):
        cache_copy(k).wait()

        def one(j, carry):
            b = 2 * (k * block // 2 + j)
            pair = jnp.concatenate([cache_v[b], cache_v[b + 1]], axis=1)
            packed[k * block // 2 + j] = jnp.dot(pair, chooser, preferred_element_type=f32).astype(bf16)
            for i in range(2):
                keys_t[pl.ds(pl.multiple_of((b + i) * head, head), head), :] = cache_v[b + i].T[:head]
            return carry

        for j in range(block//2): one(j,0)

    for k in range(EARLY):
        prepare(k)

    query_all.wait_recv()
    query_2[second_slots[0]] = total(query_1, 0, n_kv1).astype(bf16)
    query_2[second_slots[1]] = total(query_1, n_kv1, n_kv1 + n_kv0).astype(bf16)
    query_all = exchange(query_2, *second_ways)
    new_all.wait_recv()
    new_2[second_slots[0]] = total(new_1, 0, n_kv1).astype(bf16)
    new_2[second_slots[1]] = total(new_1, n_kv1, n_kv1 + n_kv0).astype(bf16)
    new_all = exchange(new_2, *second_ways)
    for k in range(EARLY, blocks):
        prepare(k)
    query_all.wait_recv()
    new_all.wait_recv()
    sums = jnp.concatenate([total(query_2, 0, n_kv0), total(query_2, n_kv0, n_kv0 + n_kv1)], axis=0)
    sum_query, gates = sums[:, : heads * head], sums[:, heads * head :]
    total_squares = gates[:, n_gates : n_gates + 1]
    row_scale = lax.rsqrt(total_squares / width + norm_eps)
    query = (row_scale * sum_query).astype(bf16).astype(f32)
    log_gate = []
    for h in range(heads):
        pick = at[2] * heads + h
        logit = jnp.sum(jnp.where(lane == pick, gates, 0.0), axis=1, keepdims=True)
        logit = row_scale * logit + bias_s[h]
        log_gate.append(jnp.minimum(logit, 0.0) - jnp.log1p(jnp.exp(-jnp.abs(logit))))
    cum_query = last_cum + jnp.concatenate(log_gate, axis=0)

    doubled = []
    for pair in range(heads // 2):
        two = query[:, pair * 128 : (pair + 1) * 128]
        turned = pltpu.roll(two, 64, 1)
        doubled.append(jnp.where(lane < head, two, turned))
        doubled.append(jnp.where(lane < head, turned, two))
    doubled = jnp.concatenate(doubled, axis=0)
    row_of = iota((rows, 128), 0) % batch
    lane_of = iota((rows, 128), 1)
    side = jnp.where(lane_of < head, 0, 1)
    inv_root = head ** (-0.5)
    scaled = doubled * inv_root
    spread = jnp.concatenate(
        [jnp.where(row_of == 2 * p + side, scaled, 0.0).astype(bf16) for p in range(batch // 2)], axis=1
    )

    tile = 256
    peak = jnp.full((rows, 128), masked_floor, f32)
    for n in range(span // tile):
        cut = slice(n * tile, (n + 1) * tile)
        score = jnp.dot(spread, keys_t[:, cut], preferred_element_type=f32) + cum_neg[:, cut]
        biased[:, cut] = score
        for k in range(tile // 128):
            peak = jnp.maximum(peak, score[:, k * 128 : (k + 1) * 128])

    new_rows = jnp.concatenate([total(new_2, 0, n_kv0), total(new_2, n_kv0, n_kv0 + n_kv1)], axis=0)
    new_rows = (row_scale * new_rows).astype(bf16).astype(f32)
    new_rows = jnp.concatenate([new_rows] * heads, axis=0)
    new_biased = (
        jnp.sum(jnp.where(lane_of < head, doubled * new_rows, 0.0), axis=1, keepdims=True) * inv_root
        - cum_query
    )

    peak = jnp.max(peak, axis=1, keepdims=True)
    peak = jnp.where(holds, jnp.maximum(peak, new_biased), peak)
    peak = jnp.maximum(peak, empty_peak)
    sums = jnp.zeros((rows, 128), f32)
    for n in range(span // 128):
        cut = slice(n * 128, (n + 1) * 128)
        weight = jnp.exp(biased[:, cut] - peak)
        sums = sums + weight
        weights[:, cut] = weight.astype(bf16)
    new_weight = jnp.where(holds, jnp.exp(new_biased - peak), 0.0)
    weight_sum = jnp.sum(sums, axis=1, keepdims=True) + new_weight

    diagonal = iota((rows, 128), 0) == lane_of

    def as_row(column):
        return jnp.sum(jnp.where(diagonal, column, 0.0), axis=0, keepdims=True)

    sub = iota((4, 128), 0)
    anchor = jnp.where(holds, cum_query, 0.0)
    stat_x[kv_index] = jnp.where(
        sub == 0, as_row(peak), jnp.where(sub == 1, as_row(weight_sum), as_row(anchor))
    )
    stat_all = exchange(stat_x, (kv_index, kv_offsets))

    values = jnp.where(lane_of < head, 0.0, new_weight.astype(bf16).astype(f32) * new_rows)
    for q in range(batch // 4):
        four = jnp.concatenate([packed[2 * q], packed[2 * q + 1]], axis=1)
        out = jnp.dot(weights[...], four, preferred_element_type=f32)
        for i in range(2):
            values = values + jnp.where(row_of == 4 * q + 2 * i + side, out[:, 128 * i : 128 * (i + 1)], 0.0)
    turned = values.T
    val_x[kv_index] = (turned[:head] + turned[head:]).astype(bf16)
    val_all = exchange(val_x, (kv_index, kv_offsets))

    wo_load.wait()
    stat_all.wait_recv()
    peaks = stat_x[:, 0, :]
    peak = jnp.max(peaks, axis=0, keepdims=True)
    factors = jnp.exp(peaks - peak)
    weight_sum = jnp.sum(stat_x[:, 1, :] * factors, axis=0, keepdims=True)
    logs = peak + jnp.log(weight_sum) + jnp.sum(stat_x[:, 2, :], axis=0, keepdims=True)
    factors = factors / weight_sum
    log_weight[...] = jnp.concatenate([logs[:, h * batch : (h + 1) * batch] for h in range(heads)], axis=0)
    val_all.wait_recv()
    acc = val_x[0].astype(f32) * factors[0:1]
    for k in range(1, n_kv):
        acc = acc + val_x[k].astype(f32) * factors[k : k + 1]
    attended = acc.T.astype(bf16)
    part_out = jnp.zeros((batch, w_out.shape[1]), f32)
    for h in range(heads):
        part_out = part_out + jnp.dot(
            attended[h * batch : (h + 1) * batch],
            wo_v[h * head : (h + 1) * head],
            preferred_element_type=f32,
        )
    out_x[at[2]] = part_out.astype(bf16)
    exchange(out_x, (at[2], tp_offsets)).wait_recv()
    acc = out_x[0].astype(f32)
    for k in range(1, n_tp):
        acc = acc + out_x[k].astype(f32)
    mixed[...] = acc.astype(bf16)
    for every in sent:
        every.wait_send()


def store(mixed, log_weight, mixed_out, log_out, sem):
    copies = [
        pltpu.make_async_copy(mixed, mixed_out, sem.at[0]),
        pltpu.make_async_copy(log_weight, log_out, sem.at[1]),
    ]
    for copy in copies:
        copy.start()
    for copy in copies:
        copy.wait()


def shards(*args):
    (tokens, gain, w_query, w_key, w_value, gate_w, gate_bias, cache, cum, lengths, w_out) = args
    n_kv0, n_kv1, n_tp = (lax.axis_size(a) for a in ("kv_0", "kv_1", "tp"))
    n_kv = n_kv0 * n_kv1
    batch, cols = tokens.shape
    span, head = cache.shape[1], cache.shape[3] // 2
    heads = cum.shape[1]
    rows = heads * batch
    half = batch // 2
    anywhere = pl.BlockSpec(memory_space=pl.ANY)
    near = pl.BlockSpec(memory_space=pltpu.VMEM)
    mixed, logs = pl.pallas_call(
        functools.partial(kernel, n_kv0, n_kv1, n_tp),
        out_shape=(
            pltpu.VMEM((batch, w_out.shape[1]), bf16),
            pltpu.VMEM((heads, batch), f32),
        ),
        in_specs=[anywhere] * len(args),
        out_specs=(near, near),
        scratch_shapes=[
            pltpu.VMEM((batch, cols), bf16),
            pltpu.VMEM((1, cols), f32),
            pltpu.VMEM(w_query.shape, bf16),
            pltpu.VMEM((2 * head, cols), bf16),
            pltpu.VMEM((128, cols), bf16),
            pltpu.VMEM(w_out.shape, bf16),
            pltpu.SMEM(gate_bias.shape, f32),
            pltpu.SMEM(lengths.shape, jnp.int32),
            pltpu.VMEM((batch, span, 2 * head), bf16),
            pltpu.VMEM(cum.shape, f32),
            pltpu.VMEM((batch * head, span), bf16),
            pltpu.VMEM((batch // 2, span, 2 * head), bf16),
            pltpu.VMEM((rows, span), f32),
            pltpu.VMEM((rows, span), f32),
            pltpu.VMEM((rows, span), bf16),
            pltpu.VMEM((n_kv0 + n_kv1, half, heads * head + 128), bf16),
            pltpu.VMEM((n_kv0 + n_kv1, half, heads * head + 128), bf16),
            pltpu.VMEM((n_kv0 + n_kv1, half, 2 * head), bf16),
            pltpu.VMEM((n_kv0 + n_kv1, half, 2 * head), bf16),
            pltpu.VMEM((n_kv, head, rows), bf16),
            pltpu.VMEM((n_kv, 4, rows), f32),
            pltpu.VMEM((n_tp, batch, w_out.shape[1]), bf16),
            pltpu.SemaphoreType.DMA((9,)),
            pltpu.SemaphoreType.DMA((7,)),
            pltpu.SemaphoreType.DMA((7,)),
        ],
        compiler_params=pltpu.CompilerParams(
            collective_id=0, has_side_effects=True, vmem_limit_bytes=60 * 1024 * 1024
        ),
    )(
        tokens,
        gain.reshape(1, cols),
        w_query,
        w_key.T,
        w_value.T,
        gate_w.T,
        gate_bias,
        cache.reshape(batch, span, 2 * head),
        cum,
        lengths,
        w_out,
    )
    mixed, logs = pl.pallas_call(
        store,
        out_shape=(jax.ShapeDtypeStruct(mixed.shape, bf16), jax.ShapeDtypeStruct(logs.shape, f32)),
        in_specs=(near, near),
        out_specs=(anywhere, anywhere),
        scratch_shapes=[pltpu.SemaphoreType.DMA((2,))],
        compiler_params=pltpu.CompilerParams(vmem_limit_bytes=1024 * 1024),
    )(mixed, logs)
    return mixed, logs.T


def solution(mesh):
    torus = Mesh(mesh.devices.reshape(4, 4, mesh.shape["tp"]), ("kv_0", "kv_1", "tp"))
    placed = (
        P(None, KV),
        P(KV),
        P(KV, "tp"),
        P(KV, "tp"),
        P(KV, "tp"),
        P(),
        P("tp"),
        P(None, KV, "tp", None),
        P(None, "tp", KV),
        P(),
        P("tp", KV),
    )
    return jax.shard_map(
        shards, mesh=torus, in_specs=placed, out_specs=(P(None, KV), P(None, "tp")), check_vma=False
    )
```

```python
import functools
import itertools

import jax
import jax.numpy as jnp
from jax import lax
from jax.experimental import pallas as pl
from jax.experimental.pallas import tpu as pltpu
from jax.sharding import Mesh
from jax.sharding import PartitionSpec as P

KV = ("kv_0", "kv_1")
MESH = pl.DeviceIdType.MESH
NT = (((1,), (1,)), ((), ()))
norm_eps = 1e-05
masked_floor = -1e30
empty_peak = -1e29
MID, SEND = 2, 6
EARLY = 1
f32, bf16 = jnp.float32, jnp.bfloat16


def iota(shape, axis):
    return lax.broadcasted_iota(jnp.int32, shape, axis)


def hops(offset, sizes):
    return sum(min(o, n - o) for o, n in zip(offset, sizes))


def kernel(
    n_kv0,
    n_kv1,
    n_tp,
    tokens,
    gain,
    w_query,
    w_key,
    w_value,
    gate_rows,
    gate_bias,
    cache,
    cum,
    lengths,
    w_out,
    mixed,
    log_weight,
    tok_v,
    gain_v,
    wq_v,
    wkv_v,
    wg_v,
    wo_v,
    bias_s,
    len_s,
    cache_v,
    cum_v,
    keys_t,
    packed,
    cum_neg,
    biased,
    weights,
    query_1,
    query_2,
    new_1,
    new_2,
    val_x,
    stat_x,
    scale,
    out_x,
    load_sem,
    send_sem,
    recv_sem,
):
    at = tuple(lax.axis_index(a) for a in ("kv_0", "kv_1", "tp"))
    sizes = (n_kv0, n_kv1, n_tp)
    n_kv = n_kv0 * n_kv1
    kv_index = at[0] * n_kv1 + at[1]
    batch, span = cache.shape[0], cache.shape[1]
    cols = tokens.shape[1]
    heads = cum.shape[1]
    head = cache.shape[2] // 2
    rows = heads * batch
    width = cols * n_kv
    n_gates = gate_rows.shape[0]

    def load(number, src, dst):
        copy = pltpu.make_async_copy(src, dst, load_sem.at[number])
        copy.start()
        return copy

    kv_offsets = [(a, b, 0) for a in range(n_kv0) for b in range(n_kv1) if a or b]
    tp_offsets = [(0, 0, c) for c in range(1, n_tp)]
    axis_offsets = ([(a, 0, 0) for a in range(1, n_kv0)], [(0, b, 0) for b in range(1, n_kv1)])
    for offsets in (kv_offsets, tp_offsets, *axis_offsets):
        offsets.sort(key=lambda o: (-hops(o, sizes), -sum(1 for c in o if c)))

    def moved(p, o, n):
        return jnp.where(p + o >= n, p + o - n, p + o) if o else p

    def peer(offset, sign=1):
        return tuple(moved(p, o if sign > 0 else (n - o) % n, n) for p, o, n in zip(at, offset, sizes))

    barrier = pltpu.get_barrier_semaphore()
    near_offsets = axis_offsets[0] + axis_offsets[1] + tp_offsets
    for offset in near_offsets:
        pl.semaphore_signal(barrier, inc=1, device_id=peer(offset), device_id_type=MESH)

    mine = gate_rows.at[:, pl.ds(pl.multiple_of(kv_index * cols, cols), cols)]
    small = [load(0, tokens, tok_v), load(0, gain, gain_v), load(0, w_query, wq_v)]
    small += [load(0, mine, wg_v.at[pl.ds(0, n_gates)])]
    small_new = [load(1, w_key, wkv_v.at[pl.ds(0, head)]), load(1, w_value, wkv_v.at[pl.ds(head, head)])]

    scalar_loads = [load(2, lengths, len_s), load(2, gate_bias, bias_s)]
    cum_load = load(3, cum, cum_v)
    blocks = 4
    block = batch // blocks

    def cache_copy(k):
        part = pl.ds(k * block, block)
        return pltpu.make_async_copy(cache.at[part], cache_v.at[part], load_sem.at[5 + k])

    for k in range(blocks):
        cache_copy(k).start()
    wo_load = load(4, w_out, wo_v)

    numbers = itertools.count()
    sent = []

    def exchange(buffer, *ways):
        number = next(numbers)
        copies = 0
        for me, offsets in ways:
            for offset in offsets:
                copies += 1
                pltpu.make_async_remote_copy(
                    src_ref=buffer.at[me],
                    dst_ref=buffer.at[me],
                    send_sem=send_sem.at[number],
                    recv_sem=recv_sem.at[number],
                    device_id=peer(offset),
                    device_id_type=MESH,
                ).start()
        others = buffer.at[pl.ds(0, copies)]
        every = pltpu.make_async_remote_copy(
            src_ref=others,
            dst_ref=others,
            send_sem=send_sem.at[number],
            recv_sem=recv_sem.at[number],
            device_id=peer(ways[0][1][0]),
            device_id_type=MESH,
        )
        sent.append(every)
        return every

    first_slots = (at[1], n_kv1 + at[0])
    first_ways = tuple(zip(first_slots, (axis_offsets[1], axis_offsets[0])))
    second_slots = (at[0], n_kv0 + at[1])
    second_ways = tuple(zip(second_slots, axis_offsets))

    def total(buffer, low, high):
        acc = buffer[low].astype(f32)
        for k in range(low + 1, high):
            acc = acc + buffer[k].astype(f32)
        return acc

    wg_v[n_gates:, :] = jnp.zeros((wg_v.shape[0] - n_gates, cols), bf16)
    for copy in small:
        copy.wait()
    tokens_f = tok_v[...].astype(f32)
    squares = jnp.sum(tokens_f * tokens_f, axis=1, keepdims=True)
    normed = (tokens_f * gain_v[...]).astype(bf16)
    lane = iota((batch, 128), 1)
    half = batch // 2
    part_query = jnp.dot(normed, wq_v[...], preferred_element_type=f32).astype(bf16)
    part_gate = lax.dot_general(normed, wg_v[...], NT, preferred_element_type=f32)
    part_gate = jnp.where(lane < n_gates, part_gate, squares).astype(bf16)
    for part in range(2):
        chunk = slice(part * half, (part + 1) * half)
        query_1[first_slots[part], :, : heads * head] = part_query[chunk]
        query_1[first_slots[part], :, heads * head :] = part_gate[chunk]

    pl.semaphore_wait(barrier, len(near_offsets))
    query_all = exchange(query_1, *first_ways)
    for copy in small_new:
        copy.wait()
    part_new = lax.dot_general(normed, wkv_v[...], NT, preferred_element_type=f32).astype(bf16)
    for part in range(2):
        new_1[first_slots[part]] = part_new[part * half : (part + 1) * half]
    new_all = exchange(new_1, *first_ways)

    for copy in scalar_loads:
        copy.wait()
    cum_load.wait()
    first_pos = kv_index * span
    length_rows = jnp.zeros((batch, 128), jnp.int32)
    for b in range(batch):
        length_rows = jnp.where(iota((batch, 128), 0) == b, len_s[b], length_rows)
    length_col = length_rows[:, :1] - first_pos
    last_parts = []
    for h in range(heads):
        last = jnp.zeros((batch, 128), f32)
        for n in range(span // 128):
            position = iota((batch, 128), 1) + n * 128
            value = cum_v[:, h, n * 128 : (n + 1) * 128]
            cum_neg[h * batch : (h + 1) * batch, n * 128 : (n + 1) * 128] = jnp.where(
                position < length_col, -value, masked_floor
            )
            last = last + jnp.where(position == length_col - 1, value, 0.0)
        last_parts.append(jnp.sum(last, axis=1, keepdims=True))
    last_cum = jnp.concatenate(last_parts, axis=0)
    holds = (length_col > 0) & (length_col <= span)
    holds = jnp.concatenate([jnp.where(holds, 1, 0)] * heads, axis=0) > 0

    column = iota((4 * head, 2 * head), 1)
    chosen = jnp.where(column < head, column + head, column + 2 * head)
    chooser = jnp.where(iota((4 * head, 2 * head), 0) == chosen, 1.0, 0.0).astype(bf16)

    def prepare(k):
        cache_copy(k).wait()

        def one(j, carry):
            b = 2 * (k * block // 2 + j)
            pair = jnp.concatenate([cache_v[b], cache_v[b + 1]], axis=1)
            packed[k * block // 2 + j] = jnp.dot(pair, chooser, preferred_element_type=f32).astype(bf16)
            for i in range(2):
                keys_t[pl.ds(pl.multiple_of((b + i) * head, head), head), :] = cache_v[b + i].T[:head]
            return carry

        for j in range(block//2): one(j,0)

    for k in range(EARLY):
        prepare(k)

    query_all.wait_recv()
    query_2[second_slots[0]] = total(query_1, 0, n_kv1).astype(bf16)
    query_2[second_slots[1]] = total(query_1, n_kv1, n_kv1 + n_kv0).astype(bf16)
    query_all = exchange(query_2, *second_ways)
    new_all.wait_recv()
    new_2[second_slots[0]] = total(new_1, 0, n_kv1).astype(bf16)
    new_2[second_slots[1]] = total(new_1, n_kv1, n_kv1 + n_kv0).astype(bf16)
    new_all = exchange(new_2, *second_ways)
    for k in range(EARLY, blocks):
        prepare(k)
    query_all.wait_recv()
    new_all.wait_recv()
    sums = jnp.concatenate([total(query_2, 0, n_kv0), total(query_2, n_kv0, n_kv0 + n_kv1)], axis=0)
    sum_query, gates = sums[:, : heads * head], sums[:, heads * head :]
    total_squares = gates[:, n_gates : n_gates + 1]
    row_scale = lax.rsqrt(total_squares / width + norm_eps)
    query = (row_scale * sum_query).astype(bf16).astype(f32)
    log_gate = []
    for h in range(heads):
        pick = at[2] * heads + h
        logit = jnp.sum(jnp.where(lane == pick, gates, 0.0), axis=1, keepdims=True)
        logit = row_scale * logit + bias_s[h]
        log_gate.append(jnp.minimum(logit, 0.0) - jnp.log1p(jnp.exp(-jnp.abs(logit))))
    cum_query = last_cum + jnp.concatenate(log_gate, axis=0)

    doubled = []
    for pair in range(heads // 2):
        two = query[:, pair * 128 : (pair + 1) * 128]
        turned = pltpu.roll(two, 64, 1)
        doubled.append(jnp.where(lane < head, two, turned))
        doubled.append(jnp.where(lane < head, turned, two))
    doubled = jnp.concatenate(doubled, axis=0)
    row_of = iota((rows, 128), 0) % batch
    lane_of = iota((rows, 128), 1)
    side = jnp.where(lane_of < head, 0, 1)
    inv_root = head ** (-0.5)
    scaled = doubled * inv_root
    spread = jnp.concatenate(
        [jnp.where(row_of == 2 * p + side, scaled, 0.0).astype(bf16) for p in range(batch // 2)], axis=1
    )

    tile = 640
    peak = jnp.full((rows, 128), masked_floor, f32)
    for n in range(span // tile):
        cut = slice(n * tile, (n + 1) * tile)
        score = jnp.dot(spread, keys_t[:, cut], preferred_element_type=f32) + cum_neg[:, cut]
        biased[:, cut] = score
        for k in range(tile // 128):
            peak = jnp.maximum(peak, score[:, k * 128 : (k + 1) * 128])

    new_rows = jnp.concatenate([total(new_2, 0, n_kv0), total(new_2, n_kv0, n_kv0 + n_kv1)], axis=0)
    new_rows = (row_scale * new_rows).astype(bf16).astype(f32)
    new_rows = jnp.concatenate([new_rows] * heads, axis=0)
    new_biased = (
        jnp.sum(jnp.where(lane_of < head, doubled * new_rows, 0.0), axis=1, keepdims=True) * inv_root
        - cum_query
    )

    peak = jnp.max(peak, axis=1, keepdims=True)
    peak = jnp.where(holds, jnp.maximum(peak, new_biased), peak)
    peak = jnp.maximum(peak, empty_peak)
    sums = jnp.zeros((rows, 128), f32)
    for n in range(span // 128):
        cut = slice(n * 128, (n + 1) * 128)
        weight = jnp.exp(biased[:, cut] - peak)
        sums = sums + weight
        weights[:, cut] = weight.astype(bf16)
    new_weight = jnp.where(holds, jnp.exp(new_biased - peak), 0.0)
    weight_sum = jnp.sum(sums, axis=1, keepdims=True) + new_weight

    values = jnp.where(lane_of < head, 0.0, new_weight.astype(bf16).astype(f32) * new_rows)

    def weigh(values, first, count):
        wide = jnp.concatenate([packed[2 * first + i] for i in range(2 * count)], axis=1)
        out = jnp.dot(weights[...], wide, preferred_element_type=f32)
        for i in range(2 * count):
            pair = 4 * first + 2 * i
            values = values + jnp.where(row_of == pair + side, out[:, 128 * i : 128 * (i + 1)], 0.0)
        return values

    quads = batch // 4
    for q in range(0, MID):
        values = weigh(values, q, 1)

    diagonal = iota((rows, 128), 0) == lane_of

    def as_row(column):
        return jnp.sum(jnp.where(diagonal, column, 0.0), axis=0, keepdims=True)

    sub = iota((4, 128), 0)
    anchor = jnp.where(holds, cum_query, 0.0)
    stat_x[kv_index] = jnp.where(
        sub == 0, as_row(peak), jnp.where(sub == 1, as_row(weight_sum), as_row(anchor))
    )
    stat_all = exchange(stat_x, (kv_index, kv_offsets))


    for q in range(MID, quads // 2):
        values = weigh(values, q, 1)

    half_lane = iota((half, 128), 1)

    def paired(column, part):
        found = []
        for h in range(0, heads, 2):
            low, high = h * batch + part * half, (h + 1) * batch + part * half
            found.append(jnp.where(half_lane < head, column[low : low + half], column[high : high + half]))
        return jnp.concatenate(found, axis=0)

    def fold(values):
        return values + pltpu.roll(values, head, 1)

    val_x[0, kv_index] = paired(fold(values), 0).astype(bf16)
    for q in range(quads // 2, SEND):
        values = weigh(values, q, 1)
    val_all = [exchange(val_x.at[0], (kv_index, kv_offsets))]
    for q in range(SEND, quads):
        values = weigh(values, q, 1)
    val_x[1, kv_index] = paired(fold(values), 1).astype(bf16)
    val_all.append(exchange(val_x.at[1], (kv_index, kv_offsets)))

    wo_load.wait()
    stat_all.wait_recv()
    peaks = stat_x[:, 0, :]
    peak = jnp.max(peaks, axis=0, keepdims=True)
    factors = jnp.exp(peaks - peak)
    weight_sum = jnp.sum(stat_x[:, 1, :] * factors, axis=0, keepdims=True)
    logs = peak + jnp.log(weight_sum) + jnp.sum(stat_x[:, 2, :], axis=0, keepdims=True)
    factors = factors / weight_sum
    log_weight[...] = jnp.concatenate([logs[:, h * batch : (h + 1) * batch] for h in range(heads)], axis=0)
    columns = factors.T
    for part in range(2):
        for k in range(n_kv):
            scale[part, k] = paired(columns[:, k : k + 1], part)
    out_all = []
    for part in range(2):
        val_all[part].wait_recv()
        acc = val_x[part, 0].astype(f32) * scale[part, 0]
        for k in range(1, n_kv):
            acc = acc + val_x[part, k].astype(f32) * scale[part, k]
        attended = jnp.concatenate([acc[i * half : (i + 1) * half] for i in range(heads // 2)], axis=1)
        part_out = jnp.dot(attended.astype(bf16), wo_v[...], preferred_element_type=f32)
        out_x[part, at[2]] = part_out.astype(bf16)
        out_all.append(exchange(out_x.at[part], (at[2], tp_offsets)))
    for part in range(2):
        out_all[part].wait_recv()
        acc = out_x[part, 0].astype(f32)
        for k in range(1, n_tp):
            acc = acc + out_x[part, k].astype(f32)
        mixed[part * half : (part + 1) * half] = acc.astype(bf16)
    for every in sent:
        every.wait_send()


def store(mixed, log_weight, mixed_out, log_out, sem):
    copies = [
        pltpu.make_async_copy(mixed, mixed_out, sem.at[0]),
        pltpu.make_async_copy(log_weight, log_out, sem.at[1]),
    ]
    for copy in copies:
        copy.start()
    for copy in copies:
        copy.wait()


def shards(*args):
    (tokens, gain, w_query, w_key, w_value, gate_w, gate_bias, cache, cum, lengths, w_out) = args
    n_kv0, n_kv1, n_tp = (lax.axis_size(a) for a in ("kv_0", "kv_1", "tp"))
    n_kv = n_kv0 * n_kv1
    batch, cols = tokens.shape
    span, head = cache.shape[1], cache.shape[3] // 2
    heads = cum.shape[1]
    rows = heads * batch
    half = batch // 2
    anywhere = pl.BlockSpec(memory_space=pl.ANY)
    near = pl.BlockSpec(memory_space=pltpu.VMEM)
    mixed, logs = pl.pallas_call(
        functools.partial(kernel, n_kv0, n_kv1, n_tp),
        out_shape=(
            pltpu.VMEM((batch, w_out.shape[1]), bf16),
            pltpu.VMEM((heads, batch), f32),
        ),
        in_specs=[anywhere] * len(args),
        out_specs=(near, near),
        scratch_shapes=[
            pltpu.VMEM((batch, cols), bf16),
            pltpu.VMEM((1, cols), f32),
            pltpu.VMEM(w_query.shape, bf16),
            pltpu.VMEM((2 * head, cols), bf16),
            pltpu.VMEM((128, cols), bf16),
            pltpu.VMEM(w_out.shape, bf16),
            pltpu.SMEM(gate_bias.shape, f32),
            pltpu.SMEM(lengths.shape, jnp.int32),
            pltpu.VMEM((batch, span, 2 * head), bf16),
            pltpu.VMEM(cum.shape, f32),
            pltpu.VMEM((batch * head, span), bf16),
            pltpu.VMEM((batch // 2, span, 2 * head), bf16),
            pltpu.VMEM((rows, span), f32),
            pltpu.VMEM((rows, span), f32),
            pltpu.VMEM((rows, span), bf16),
            pltpu.VMEM((n_kv0 + n_kv1, half, heads * head + 128), bf16),
            pltpu.VMEM((n_kv0 + n_kv1, half, heads * head + 128), bf16),
            pltpu.VMEM((n_kv0 + n_kv1, half, 2 * head), bf16),
            pltpu.VMEM((n_kv0 + n_kv1, half, 2 * head), bf16),
            pltpu.VMEM((2, n_kv, rows // 4, 2 * head), bf16),
            pltpu.VMEM((n_kv, 4, rows), f32),
            pltpu.VMEM((2, n_kv, rows // 4, 2 * head), f32),
            pltpu.VMEM((2, n_tp, half, w_out.shape[1]), bf16),
            pltpu.SemaphoreType.DMA((9,)),
            pltpu.SemaphoreType.DMA((9,)),
            pltpu.SemaphoreType.DMA((9,)),
        ],
        compiler_params=pltpu.CompilerParams(
            collective_id=0, has_side_effects=True, vmem_limit_bytes=60 * 1024 * 1024
        ),
    )(
        tokens,
        gain.reshape(1, cols),
        w_query,
        w_key.T,
        w_value.T,
        gate_w.T,
        gate_bias,
        cache.reshape(batch, span, 2 * head),
        cum,
        lengths,
        w_out,
    )
    mixed, logs = pl.pallas_call(
        store,
        out_shape=(jax.ShapeDtypeStruct(mixed.shape, bf16), jax.ShapeDtypeStruct(logs.shape, f32)),
        in_specs=(near, near),
        out_specs=(anywhere, anywhere),
        scratch_shapes=[pltpu.SemaphoreType.DMA((2,))],
        compiler_params=pltpu.CompilerParams(vmem_limit_bytes=1024 * 1024),
    )(mixed, logs)
    return mixed, logs.T


def solution(mesh):
    torus = Mesh(mesh.devices.reshape(4, 4, mesh.shape["tp"]), ("kv_0", "kv_1", "tp"))
    placed = (
        P(None, KV),
        P(KV),
        P(KV, "tp"),
        P(KV, "tp"),
        P(KV, "tp"),
        P(),
        P("tp"),
        P(None, KV, "tp", None),
        P(None, "tp", KV),
        P(),
        P("tp", KV),
    )
    return jax.shard_map(
        shards, mesh=torus, in_specs=placed, out_specs=(P(None, KV), P(None, "tp")), check_vma=False
    )
```

```python
import functools
import itertools

import jax
import jax.numpy as jnp
from jax import lax
from jax.experimental import pallas as pl
from jax.experimental.pallas import tpu as pltpu
from jax.sharding import Mesh
from jax.sharding import PartitionSpec as P

KV = ("kv_0", "kv_1")
MESH = pl.DeviceIdType.MESH
NT = (((1,), (1,)), ((), ()))
norm_eps = 1e-05
masked_floor = -1e30
empty_peak = -1e29
SEGMENTS = ((0, 512), (512, 1024), (1024, 1280))
WIDEST = 640
MID, SEND = 4, 6
EARLY = 1
f32, bf16 = jnp.float32, jnp.bfloat16


def iota(shape, axis):
    return lax.broadcasted_iota(jnp.int32, shape, axis)


def hops(offset, sizes):
    return sum(min(o, n - o) for o, n in zip(offset, sizes))


def cuts(low, high):
    steps = -(-(high - low) // WIDEST)
    step = -(-(high - low) // steps // 128) * 128
    return [slice(k, min(k + step, high)) for k in range(low, high, step)]


def kernel(
    n_kv0,
    n_kv1,
    n_tp,
    tokens,
    gain,
    w_query,
    w_key,
    w_value,
    gate_rows,
    gate_bias,
    cache,
    cum,
    lengths,
    w_out,
    mixed,
    log_weight,
    tok_v,
    gain_v,
    wq_v,
    wkv_v,
    wg_v,
    wo_v,
    bias_s,
    len_s,
    cache_v,
    cum_v,
    keys_t,
    packed,
    cum_neg,
    biased,
    weights,
    query_1,
    query_2,
    new_1,
    new_2,
    val_x,
    stat_x,
    scale,
    out_x,
    load_sem,
    send_sem,
    recv_sem,
):
    at = tuple(lax.axis_index(a) for a in ("kv_0", "kv_1", "tp"))
    sizes = (n_kv0, n_kv1, n_tp)
    n_kv = n_kv0 * n_kv1
    kv_index = at[0] * n_kv1 + at[1]
    batch, span = cache.shape[0], cache.shape[1]
    cols = tokens.shape[1]
    heads = cum.shape[1]
    head = cache.shape[2] // 2
    rows = heads * batch
    width = cols * n_kv
    n_gates = gate_rows.shape[0]

    def load(number, src, dst):
        copy = pltpu.make_async_copy(src, dst, load_sem.at[number])
        copy.start()
        return copy

    kv_offsets = [(a, b, 0) for a in range(n_kv0) for b in range(n_kv1) if a or b]
    tp_offsets = [(0, 0, c) for c in range(1, n_tp)]
    axis_offsets = ([(a, 0, 0) for a in range(1, n_kv0)], [(0, b, 0) for b in range(1, n_kv1)])
    for offsets in (kv_offsets, tp_offsets, *axis_offsets):
        offsets.sort(key=lambda o: (-hops(o, sizes), -sum(1 for c in o if c)))

    def moved(p, o, n):
        return jnp.where(p + o >= n, p + o - n, p + o) if o else p

    def peer(offset, sign=1):
        return tuple(moved(p, o if sign > 0 else (n - o) % n, n) for p, o, n in zip(at, offset, sizes))

    barrier = pltpu.get_barrier_semaphore()
    near_offsets = axis_offsets[0] + axis_offsets[1] + tp_offsets
    near_offsets.sort(key=lambda o: -hops(o, sizes))
    for offset in near_offsets:
        pl.semaphore_signal(barrier, inc=1, device_id=peer(offset), device_id_type=MESH)

    mine = gate_rows.at[:, pl.ds(pl.multiple_of(kv_index * cols, cols), cols)]
    small = [load(0, tokens, tok_v), load(0, gain, gain_v), load(0, w_query, wq_v)]
    small += [load(0, mine, wg_v.at[pl.ds(0, n_gates)])]
    small_new = [load(1, w_key, wkv_v.at[pl.ds(0, head)]), load(1, w_value, wkv_v.at[pl.ds(head, head)])]

    scalar_loads = [load(2, lengths, len_s), load(2, gate_bias, bias_s)]
    cum_load = load(3, cum, cum_v)
    blocks = 4
    block = batch // blocks

    def cache_copy(k):
        part = pl.ds(k * block, block)
        return pltpu.make_async_copy(cache.at[part], cache_v.at[part], load_sem.at[5 + k])

    for k in range(blocks):
        cache_copy(k).start()
    wo_load = load(4, w_out, wo_v)

    numbers = itertools.count()
    sent = []

    def exchange(buffer, *ways):
        number = next(numbers)
        copies = 0
        for me, offsets in ways:
            for offset in offsets:
                copies += 1
                pltpu.make_async_remote_copy(
                    src_ref=buffer.at[me],
                    dst_ref=buffer.at[me],
                    send_sem=send_sem.at[number],
                    recv_sem=recv_sem.at[number],
                    device_id=peer(offset),
                    device_id_type=MESH,
                ).start()
        others = buffer.at[pl.ds(0, copies)]
        every = pltpu.make_async_remote_copy(
            src_ref=others,
            dst_ref=others,
            send_sem=send_sem.at[number],
            recv_sem=recv_sem.at[number],
            device_id=peer(ways[0][1][0]),
            device_id_type=MESH,
        )
        sent.append(every)
        return every

    first_slots = (at[1], n_kv1 + at[0])
    first_ways = tuple(zip(first_slots, (axis_offsets[1], axis_offsets[0])))
    second_slots = (at[0], n_kv0 + at[1])
    second_ways = tuple(zip(second_slots, axis_offsets))

    def total(buffer, low, high):
        acc = buffer[low].astype(f32)
        for k in range(low + 1, high):
            acc = acc + buffer[k].astype(f32)
        return acc

    wg_v[n_gates:, :] = jnp.zeros((wg_v.shape[0] - n_gates, cols), bf16)
    for copy in small:
        copy.wait()
    tokens_f = tok_v[...].astype(f32)
    squares = jnp.sum(tokens_f * tokens_f, axis=1, keepdims=True)
    normed = (tokens_f * gain_v[...]).astype(bf16)
    lane = iota((batch, 128), 1)
    half = batch // 2
    part_query = jnp.dot(normed, wq_v[...], preferred_element_type=f32).astype(bf16)
    part_gate = lax.dot_general(normed, wg_v[...], NT, preferred_element_type=f32)
    part_gate = jnp.where(lane < n_gates, part_gate, squares).astype(bf16)
    for part in range(2):
        chunk = slice(part * half, (part + 1) * half)
        query_1[first_slots[part], :, : heads * head] = part_query[chunk]
        query_1[first_slots[part], :, heads * head :] = part_gate[chunk]

    pl.semaphore_wait(barrier, len(near_offsets))
    query_all = exchange(query_1, *first_ways)
    for copy in small_new:
        copy.wait()
    part_new = lax.dot_general(normed, wkv_v[...], NT, preferred_element_type=f32).astype(bf16)
    for part in range(2):
        new_1[first_slots[part]] = part_new[part * half : (part + 1) * half]
    new_all = exchange(new_1, *first_ways)

    for copy in scalar_loads:
        copy.wait()
    cum_load.wait()
    first_pos = kv_index * span
    length_rows = jnp.zeros((batch, 128), jnp.int32)
    for b in range(batch):
        length_rows = jnp.where(iota((batch, 128), 0) == b, len_s[b], length_rows)
    length_col = length_rows[:, :1] - first_pos
    last_parts = []
    for h in range(heads):
        last = jnp.zeros((batch, 128), f32)
        for n in range(span // 128):
            position = iota((batch, 128), 1) + n * 128
            value = cum_v[:, h, n * 128 : (n + 1) * 128]
            cum_neg[h * batch : (h + 1) * batch, n * 128 : (n + 1) * 128] = jnp.where(
                position < length_col, -value, masked_floor
            )
            last = last + jnp.where(position == length_col - 1, value, 0.0)
        last_parts.append(jnp.sum(last, axis=1, keepdims=True))
    last_cum = jnp.concatenate(last_parts, axis=0)
    holds = (length_col > 0) & (length_col <= span)
    holds = jnp.concatenate([jnp.where(holds, 1, 0)] * heads, axis=0) > 0

    column = iota((4 * head, 2 * head), 1)
    chosen = jnp.where(column < head, column + head, column + 2 * head)
    chooser = jnp.where(iota((4 * head, 2 * head), 0) == chosen, 1.0, 0.0).astype(bf16)

    def prepare(k):
        cache_copy(k).wait()

        def one(j, carry):
            b = 2 * (k * block // 2 + j)
            pair = jnp.concatenate([cache_v[b], cache_v[b + 1]], axis=1)
            packed[k * block // 2 + j] = jnp.dot(pair, chooser, preferred_element_type=f32).astype(bf16)
            for i in range(2):
                keys_t[pl.ds(pl.multiple_of((b + i) * head, head), head), :] = cache_v[b + i].T[:head]
            return carry

        for j in range(block//2): one(j,0)

    for k in range(EARLY):
        prepare(k)

    query_all.wait_recv()
    query_2[second_slots[0]] = total(query_1, 0, n_kv1).astype(bf16)
    query_2[second_slots[1]] = total(query_1, n_kv1, n_kv1 + n_kv0).astype(bf16)
    query_all = exchange(query_2, *second_ways)
    new_all.wait_recv()
    new_2[second_slots[0]] = total(new_1, 0, n_kv1).astype(bf16)
    new_2[second_slots[1]] = total(new_1, n_kv1, n_kv1 + n_kv0).astype(bf16)
    new_all = exchange(new_2, *second_ways)
    for k in range(EARLY, blocks):
        prepare(k)
    query_all.wait_recv()
    new_all.wait_recv()
    sums = jnp.concatenate([total(query_2, 0, n_kv0), total(query_2, n_kv0, n_kv0 + n_kv1)], axis=0)
    sum_query, gates = sums[:, : heads * head], sums[:, heads * head :]
    total_squares = gates[:, n_gates : n_gates + 1]
    row_scale = lax.rsqrt(total_squares / width + norm_eps)
    query = (row_scale * sum_query).astype(bf16).astype(f32)
    log_gate = []
    for h in range(heads):
        pick = at[2] * heads + h
        logit = jnp.sum(jnp.where(lane == pick, gates, 0.0), axis=1, keepdims=True)
        logit = row_scale * logit + bias_s[h]
        log_gate.append(jnp.minimum(logit, 0.0) - jnp.log1p(jnp.exp(-jnp.abs(logit))))
    cum_query = last_cum + jnp.concatenate(log_gate, axis=0)

    doubled = []
    for pair in range(heads // 2):
        two = query[:, pair * 128 : (pair + 1) * 128]
        turned = pltpu.roll(two, 64, 1)
        doubled.append(jnp.where(lane < head, two, turned))
        doubled.append(jnp.where(lane < head, turned, two))
    doubled = jnp.concatenate(doubled, axis=0)
    row_of = iota((rows, 128), 0) % batch
    lane_of = iota((rows, 128), 1)
    side = jnp.where(lane_of < head, 0, 1)
    inv_root = head ** (-0.5)
    scaled = doubled * inv_root
    spread = jnp.concatenate(
        [jnp.where(row_of == 2 * p + side, scaled, 0.0).astype(bf16) for p in range(batch // 2)], axis=1
    )

    peaks, sums = [], []
    for low, high in SEGMENTS:
        top = jnp.full((rows, 128), masked_floor, f32)
        for cut in cuts(low, high):
            score = jnp.dot(spread, keys_t[:, cut], preferred_element_type=f32) + cum_neg[:, cut]
            biased[:, cut] = score
            for k in range(score.shape[1] // 128):
                top = jnp.maximum(top, score[:, k * 128 : (k + 1) * 128])
        top = jnp.maximum(jnp.max(top, axis=1, keepdims=True), empty_peak)
        part_sum = jnp.zeros((rows, 128), f32)
        for k in range(low, high, 128):
            weight = jnp.exp(biased[:, k : k + 128] - top)
            part_sum = part_sum + weight
            weights[:, k : k + 128] = weight.astype(bf16)
        peaks.append(top)
        sums.append(jnp.sum(part_sum, axis=1, keepdims=True))

    new_rows = jnp.concatenate([total(new_2, 0, n_kv0), total(new_2, n_kv0, n_kv0 + n_kv1)], axis=0)
    new_rows = (row_scale * new_rows).astype(bf16).astype(f32)
    new_rows = jnp.concatenate([new_rows] * heads, axis=0)
    new_biased = (
        jnp.sum(jnp.where(lane_of < head, doubled * new_rows, 0.0), axis=1, keepdims=True) * inv_root
        - cum_query
    )

    peak = functools.reduce(jnp.maximum, peaks)
    peak = jnp.where(holds, jnp.maximum(peak, new_biased), peak)
    shrink = [jnp.exp(p - peak) for p in peaks]
    new_weight = jnp.where(holds, jnp.exp(new_biased - peak), 0.0)
    weight_sum = sum(s * f for s, f in zip(sums, shrink)) + new_weight

    found = [jnp.zeros((rows, 128), f32) for _ in SEGMENTS]

    def weigh(segment, q):
        low, high = SEGMENTS[segment]
        four = jnp.concatenate([packed[2 * q + i, low:high] for i in range(2)], axis=1)
        out = jnp.dot(weights[:, low:high], four, preferred_element_type=f32)
        for i in range(2):
            pair = 4 * q + 2 * i
            found[segment] = found[segment] + jnp.where(
                row_of == pair + side, out[:, 128 * i : 128 * (i + 1)], 0.0
            )

    def joined():
        values = jnp.where(lane_of < head, 0.0, new_weight.astype(bf16).astype(f32) * new_rows)
        for f, v in zip(shrink, found):
            values = values + f * v
        return values + pltpu.roll(values, head, 1)

    quads = batch // 4
    last = len(SEGMENTS) - 1
    for segment in range(last):
        for q in range(quads):
            weigh(segment, q)
    for q in range(0, MID):
        weigh(last, q)

    diagonal = iota((rows, 128), 0) == lane_of

    def as_row(column):
        return jnp.sum(jnp.where(diagonal, column, 0.0), axis=0, keepdims=True)

    sub = iota((4, 128), 0)
    anchor = jnp.where(holds, cum_query, 0.0)
    stat_x[kv_index] = jnp.where(
        sub == 0, as_row(peak), jnp.where(sub == 1, as_row(weight_sum), as_row(anchor))
    )
    stat_all = exchange(stat_x, (kv_index, kv_offsets))


    for q in range(MID, quads // 2):
        weigh(last, q)

    half_lane = iota((half, 128), 1)

    def paired(column, part):
        found = []
        for h in range(0, heads, 2):
            low, high = h * batch + part * half, (h + 1) * batch + part * half
            found.append(jnp.where(half_lane < head, column[low : low + half], column[high : high + half]))
        return jnp.concatenate(found, axis=0)

    val_x[0, kv_index] = paired(joined(), 0).astype(bf16)
    for q in range(quads // 2, SEND):
        weigh(last, q)
    val_all = [exchange(val_x.at[0], (kv_index, kv_offsets))]
    for q in range(SEND, quads):
        weigh(last, q)
    val_x[1, kv_index] = paired(joined(), 1).astype(bf16)
    val_all.append(exchange(val_x.at[1], (kv_index, kv_offsets)))

    wo_load.wait()
    stat_all.wait_recv()
    peaks = stat_x[:, 0, :]
    peak = jnp.max(peaks, axis=0, keepdims=True)
    factors = jnp.exp(peaks - peak)
    weight_sum = jnp.sum(stat_x[:, 1, :] * factors, axis=0, keepdims=True)
    logs = peak + jnp.log(weight_sum) + jnp.sum(stat_x[:, 2, :], axis=0, keepdims=True)
    factors = factors / weight_sum
    log_weight[...] = jnp.concatenate([logs[:, h * batch : (h + 1) * batch] for h in range(heads)], axis=0)
    columns = factors.T
    for part in range(2):
        for k in range(n_kv):
            scale[part, k] = paired(columns[:, k : k + 1], part)
    out_all = []
    for part in range(2):
        val_all[part].wait_recv()
        acc = val_x[part, 0].astype(f32) * scale[part, 0]
        for k in range(1, n_kv):
            acc = acc + val_x[part, k].astype(f32) * scale[part, k]
        attended = jnp.concatenate([acc[i * half : (i + 1) * half] for i in range(heads // 2)], axis=1)
        part_out = jnp.dot(attended.astype(bf16), wo_v[...], preferred_element_type=f32)
        out_x[part, at[2]] = part_out.astype(bf16)
        out_all.append(exchange(out_x.at[part], (at[2], tp_offsets)))
    for part in range(2):
        out_all[part].wait_recv()
        acc = out_x[part, 0].astype(f32)
        for k in range(1, n_tp):
            acc = acc + out_x[part, k].astype(f32)
        mixed[part * half : (part + 1) * half] = acc.astype(bf16)
    for every in sent:
        every.wait_send()


def store(mixed, log_weight, mixed_out, log_out, sem):
    copies = [
        pltpu.make_async_copy(mixed, mixed_out, sem.at[0]),
        pltpu.make_async_copy(log_weight, log_out, sem.at[1]),
    ]
    for copy in copies:
        copy.start()
    for copy in copies:
        copy.wait()


def shards(*args):
    (tokens, gain, w_query, w_key, w_value, gate_w, gate_bias, cache, cum, lengths, w_out) = args
    n_kv0, n_kv1, n_tp = (lax.axis_size(a) for a in ("kv_0", "kv_1", "tp"))
    n_kv = n_kv0 * n_kv1
    batch, cols = tokens.shape
    span, head = cache.shape[1], cache.shape[3] // 2
    heads = cum.shape[1]
    rows = heads * batch
    half = batch // 2
    anywhere = pl.BlockSpec(memory_space=pl.ANY)
    near = pl.BlockSpec(memory_space=pltpu.VMEM)
    mixed, logs = pl.pallas_call(
        functools.partial(kernel, n_kv0, n_kv1, n_tp),
        out_shape=(
            pltpu.VMEM((batch, w_out.shape[1]), bf16),
            pltpu.VMEM((heads, batch), f32),
        ),
        in_specs=[anywhere] * len(args),
        out_specs=(near, near),
        scratch_shapes=[
            pltpu.VMEM((batch, cols), bf16),
            pltpu.VMEM((1, cols), f32),
            pltpu.VMEM(w_query.shape, bf16),
            pltpu.VMEM((2 * head, cols), bf16),
            pltpu.VMEM((128, cols), bf16),
            pltpu.VMEM(w_out.shape, bf16),
            pltpu.SMEM(gate_bias.shape, f32),
            pltpu.SMEM(lengths.shape, jnp.int32),
            pltpu.VMEM((batch, span, 2 * head), bf16),
            pltpu.VMEM(cum.shape, f32),
            pltpu.VMEM((batch * head, span), bf16),
            pltpu.VMEM((batch // 2, span, 2 * head), bf16),
            pltpu.VMEM((rows, span), f32),
            pltpu.VMEM((rows, span), f32),
            pltpu.VMEM((rows, span), bf16),
            pltpu.VMEM((n_kv0 + n_kv1, half, heads * head + 128), bf16),
            pltpu.VMEM((n_kv0 + n_kv1, half, heads * head + 128), bf16),
            pltpu.VMEM((n_kv0 + n_kv1, half, 2 * head), bf16),
            pltpu.VMEM((n_kv0 + n_kv1, half, 2 * head), bf16),
            pltpu.VMEM((2, n_kv, rows // 4, 2 * head), bf16),
            pltpu.VMEM((n_kv, 4, rows), f32),
            pltpu.VMEM((2, n_kv, rows // 4, 2 * head), f32),
            pltpu.VMEM((2, n_tp, half, w_out.shape[1]), bf16),
            pltpu.SemaphoreType.DMA((9,)),
            pltpu.SemaphoreType.DMA((9,)),
            pltpu.SemaphoreType.DMA((9,)),
        ],
        compiler_params=pltpu.CompilerParams(
            collective_id=0, has_side_effects=True, vmem_limit_bytes=60 * 1024 * 1024
        ),
    )(
        tokens,
        gain.reshape(1, cols),
        w_query,
        w_key.T,
        w_value.T,
        gate_w.T,
        gate_bias,
        cache.reshape(batch, span, 2 * head),
        cum,
        lengths,
        w_out,
    )
    mixed, logs = pl.pallas_call(
        store,
        out_shape=(jax.ShapeDtypeStruct(mixed.shape, bf16), jax.ShapeDtypeStruct(logs.shape, f32)),
        in_specs=(near, near),
        out_specs=(anywhere, anywhere),
        scratch_shapes=[pltpu.SemaphoreType.DMA((2,))],
        compiler_params=pltpu.CompilerParams(vmem_limit_bytes=1024 * 1024),
    )(mixed, logs)
    return mixed, logs.T


def solution(mesh):
    torus = Mesh(mesh.devices.reshape(4, 4, mesh.shape["tp"]), ("kv_0", "kv_1", "tp"))
    placed = (
        P(None, KV),
        P(KV),
        P(KV, "tp"),
        P(KV, "tp"),
        P(KV, "tp"),
        P(),
        P("tp"),
        P(None, KV, "tp", None),
        P(None, "tp", KV),
        P(),
        P("tp", KV),
    )
    return jax.shard_map(
        shards, mesh=torus, in_specs=placed, out_specs=(P(None, KV), P(None, "tp")), check_vma=False
    )
```

```python
import functools
import itertools

import jax
import jax.numpy as jnp
from jax import lax
from jax.experimental import pallas as pl
from jax.experimental.pallas import tpu as pltpu
from jax.sharding import Mesh
from jax.sharding import PartitionSpec as P

KV = ("kv_0", "kv_1")
MESH = pl.DeviceIdType.MESH
NT = (((1,), (1,)), ((), ()))
norm_eps = 1e-05
masked_floor = -1e30
empty_peak = -1e29
SEGMENTS = ((0, 512), (512, 1024), (1024, 1280))
WIDEST = 640
MID, SEND = 4, 6
EARLY = 1
f32, bf16 = jnp.float32, jnp.bfloat16


def iota(shape, axis):
    return lax.broadcasted_iota(jnp.int32, shape, axis)


def hops(offset, sizes):
    return sum(min(o, n - o) for o, n in zip(offset, sizes))


def cuts(low, high):
    steps = -(-(high - low) // WIDEST)
    step = -(-(high - low) // steps // 128) * 128
    return [slice(k, min(k + step, high)) for k in range(low, high, step)]


def kernel(
    n_kv0,
    n_kv1,
    n_tp,
    tokens,
    gain,
    w_query,
    w_key,
    w_value,
    gate_rows,
    gate_bias,
    cache,
    cum,
    lengths,
    w_out,
    mixed,
    log_weight,
    tok_v,
    gain_v,
    wq_v,
    wkv_v,
    wg_v,
    wo_v,
    bias_s,
    len_s,
    cache_v,
    cum_v,
    keys_t,
    packed,
    cum_neg,
    biased,
    weights,
    query_1,
    query_2,
    val_x,
    stat_x,
    scale,
    out_x,
    load_sem,
    send_sem,
    recv_sem,
):
    at = tuple(lax.axis_index(a) for a in ("kv_0", "kv_1", "tp"))
    sizes = (n_kv0, n_kv1, n_tp)
    n_kv = n_kv0 * n_kv1
    kv_index = at[0] * n_kv1 + at[1]
    batch, span = cache.shape[0], cache.shape[1]
    cols = tokens.shape[1]
    heads = cum.shape[1]
    head = cache.shape[2] // 2
    rows = heads * batch
    width = cols * n_kv
    n_gates = gate_rows.shape[0]

    def load(number, src, dst):
        copy = pltpu.make_async_copy(src, dst, load_sem.at[number])
        copy.start()
        return copy

    kv_offsets = [(a, b, 0) for a in range(n_kv0) for b in range(n_kv1) if a or b]
    tp_offsets = [(0, 0, c) for c in range(1, n_tp)]
    axis_offsets = ([(a, 0, 0) for a in range(1, n_kv0)], [(0, b, 0) for b in range(1, n_kv1)])
    for offsets in (kv_offsets, tp_offsets, *axis_offsets):
        offsets.sort(key=lambda o: (-hops(o, sizes), -sum(1 for c in o if c)))

    def moved(p, o, n):
        return jnp.where(p + o >= n, p + o - n, p + o) if o else p

    def peer(offset, sign=1):
        return tuple(moved(p, o if sign > 0 else (n - o) % n, n) for p, o, n in zip(at, offset, sizes))

    barrier = pltpu.get_barrier_semaphore()
    near_offsets = axis_offsets[0] + axis_offsets[1] + tp_offsets
    near_offsets.sort(key=lambda o: -hops(o, sizes))
    for offset in near_offsets:
        pl.semaphore_signal(barrier, inc=1, device_id=peer(offset), device_id_type=MESH)

    mine = gate_rows.at[:, pl.ds(pl.multiple_of(kv_index * cols, cols), cols)]
    small = [load(0, tokens, tok_v), load(0, gain, gain_v), load(0, w_query, wq_v)]
    small += [load(0, mine, wg_v.at[pl.ds(0, n_gates)])]
    small_new = [load(1, w_key, wkv_v.at[pl.ds(0, head)]), load(1, w_value, wkv_v.at[pl.ds(head, head)])]

    scalar_loads = [load(1, lengths, len_s), load(1, gate_bias, bias_s)]
    cum_load = load(2, cum, cum_v)
    wo_load = load(2, w_out, wo_v)
    blocks = 4
    block = batch // blocks

    def cache_copy(k):
        part = pl.ds(k * block, block)
        return pltpu.make_async_copy(cache.at[part], cache_v.at[part], load_sem.at[3 + k])

    for k in range(blocks):
        cache_copy(k).start()

    numbers = itertools.count()
    sent = []

    def exchange(buffer, *ways):
        number = next(numbers)
        copies = 0
        for me, offsets in ways:
            for offset in offsets:
                copies += 1
                pltpu.make_async_remote_copy(
                    src_ref=buffer.at[me],
                    dst_ref=buffer.at[me],
                    send_sem=send_sem.at[0],
                    recv_sem=recv_sem.at[number],
                    device_id=peer(offset),
                    device_id_type=MESH,
                ).start()
        others = buffer.at[pl.ds(0, copies)]
        every = pltpu.make_async_remote_copy(
            src_ref=others,
            dst_ref=others,
            send_sem=send_sem.at[0],
            recv_sem=recv_sem.at[number],
            device_id=peer(ways[0][1][0]),
            device_id_type=MESH,
        )
        sent.append(every)
        return every

    first_slots = (at[1], n_kv1 + at[0])
    first_ways = tuple(zip(first_slots, (axis_offsets[1], axis_offsets[0])))
    second_slots = (at[0], n_kv0 + at[1])
    second_ways = tuple(zip(second_slots, axis_offsets))

    def total(buffer, low, high):
        acc = buffer[low].astype(f32)
        for k in range(low + 1, high):
            acc = acc + buffer[k].astype(f32)
        return acc

    wg_v[n_gates:, :] = jnp.zeros((wg_v.shape[0] - n_gates, cols), bf16)
    for copy in small:
        copy.wait()
    tokens_f = tok_v[...].astype(f32)
    squares = jnp.sum(tokens_f * tokens_f, axis=1, keepdims=True)
    normed = (tokens_f * gain_v[...]).astype(bf16)
    lane = iota((batch, 128), 1)
    half = batch // 2
    part_query = jnp.dot(normed, wq_v[...], preferred_element_type=f32).astype(bf16)
    part_gate = lax.dot_general(normed, wg_v[...], NT, preferred_element_type=f32)
    part_gate = jnp.where(lane < n_gates, part_gate, squares).astype(bf16)
    for copy in small_new + scalar_loads:
        copy.wait()
    part_new = lax.dot_general(normed, wkv_v[...], NT, preferred_element_type=f32).astype(bf16)
    new_at = heads * head + 128
    for part in range(2):
        chunk = slice(part * half, (part + 1) * half)
        query_1[first_slots[part], :, new_at:] = part_new[chunk]
        query_1[first_slots[part], :, : heads * head] = part_query[chunk]
        query_1[first_slots[part], :, heads * head : new_at] = part_gate[chunk]

    pl.semaphore_wait(barrier, len(near_offsets))
    query_all = exchange(query_1, *first_ways)
    cum_load.wait()
    wo_load.wait()
    first_pos = kv_index * span
    length_rows = jnp.zeros((batch, 128), jnp.int32)
    for b in range(batch):
        length_rows = jnp.where(iota((batch, 128), 0) == b, len_s[b], length_rows)
    length_col = length_rows[:, :1] - first_pos
    last_parts = []
    for h in range(heads):
        last = jnp.zeros((batch, 128), f32)
        for n in range(span // 128):
            position = iota((batch, 128), 1) + n * 128
            value = cum_v[:, h, n * 128 : (n + 1) * 128]
            cum_neg[h * batch : (h + 1) * batch, n * 128 : (n + 1) * 128] = jnp.where(
                position < length_col, -value, masked_floor
            )
            last = last + jnp.where(position == length_col - 1, value, 0.0)
        last_parts.append(jnp.sum(last, axis=1, keepdims=True))
    last_cum = jnp.concatenate(last_parts, axis=0)
    holds = (length_col > 0) & (length_col <= span)
    holds = jnp.concatenate([jnp.where(holds, 1, 0)] * heads, axis=0) > 0

    column = iota((4 * head, 2 * head), 1)
    chosen = jnp.where(column < head, column + head, column + 2 * head)
    chooser = jnp.where(iota((4 * head, 2 * head), 0) == chosen, 1.0, 0.0).astype(bf16)

    def prepare(k):
        cache_copy(k).wait()

        def one(j, carry):
            b = 2 * (k * block // 2 + j)
            pair = jnp.concatenate([cache_v[b], cache_v[b + 1]], axis=1)
            packed[k * block // 2 + j] = jnp.dot(pair, chooser, preferred_element_type=f32).astype(bf16)
            for i in range(2):
                keys_t[pl.ds(pl.multiple_of((b + i) * head, head), head), :] = cache_v[b + i].T[:head]
            return carry

        for j in range(block//2): one(j,0)

    for k in range(EARLY):
        prepare(k)

    query_all.wait_recv()
    query_2[second_slots[0]] = total(query_1, 0, n_kv1).astype(bf16)
    query_2[second_slots[1]] = total(query_1, n_kv1, n_kv1 + n_kv0).astype(bf16)
    query_all = exchange(query_2, *second_ways)
    for k in range(EARLY, blocks):
        prepare(k)
    query_all.wait_recv()
    sums = jnp.concatenate([total(query_2, 0, n_kv0), total(query_2, n_kv0, n_kv0 + n_kv1)], axis=0)
    sum_query, gates, sum_new = sums[:, : heads * head], sums[:, heads * head : new_at], sums[:, new_at:]
    total_squares = gates[:, n_gates : n_gates + 1]
    row_scale = lax.rsqrt(total_squares / width + norm_eps)
    query = sum_query.astype(bf16).astype(f32)
    log_gate = []
    for h in range(heads):
        pick = at[2] * heads + h
        logit = jnp.sum(jnp.where(lane == pick, gates, 0.0), axis=1, keepdims=True)
        logit = row_scale * logit + bias_s[h]
        log_gate.append(jnp.minimum(logit, 0.0) - jnp.log1p(jnp.exp(-jnp.abs(logit))))
    cum_query = last_cum + jnp.concatenate(log_gate, axis=0)

    doubled = []
    for pair in range(heads // 2):
        two = query[:, pair * 128 : (pair + 1) * 128]
        turned = pltpu.roll(two, 64, 1)
        doubled.append(jnp.where(lane < head, two, turned))
        doubled.append(jnp.where(lane < head, turned, two))
    doubled = jnp.concatenate(doubled, axis=0)
    row_of = iota((rows, 128), 0) % batch
    lane_of = iota((rows, 128), 1)
    side = jnp.where(lane_of < head, 0, 1)
    inv_root = head ** (-0.5)
    scaled = doubled
    row_factor = jnp.concatenate([row_scale] * heads, axis=0) * inv_root
    spread = jnp.concatenate(
        [jnp.where(row_of == 2 * p + side, scaled, 0.0).astype(bf16) for p in range(batch // 2)], axis=1
    )

    peaks, sums = [], []
    for low, high in SEGMENTS:
        top = jnp.full((rows, 128), masked_floor, f32)
        for cut in cuts(low, high):
            score = jnp.dot(spread, keys_t[:, cut], preferred_element_type=f32) * row_factor + cum_neg[:, cut]
            biased[:, cut] = score
            for k in range(score.shape[1] // 128):
                top = jnp.maximum(top, score[:, k * 128 : (k + 1) * 128])
        top = jnp.maximum(jnp.max(top, axis=1, keepdims=True), empty_peak)
        part_sum = jnp.zeros((rows, 128), f32)
        for k in range(low, high, 128):
            weight = jnp.exp(biased[:, k : k + 128] - top)
            part_sum = part_sum + weight
            weights[:, k : k + 128] = weight.astype(bf16)
        peaks.append(top)
        sums.append(jnp.sum(part_sum, axis=1, keepdims=True))

    new_rows = sum_new
    new_rows = (row_scale * new_rows).astype(bf16).astype(f32)
    new_rows = jnp.concatenate([new_rows] * heads, axis=0)
    new_biased = (
        jnp.sum(jnp.where(lane_of < head, doubled * new_rows, 0.0), axis=1, keepdims=True) * row_factor
        - cum_query
    )

    peak = functools.reduce(jnp.maximum, peaks)
    peak = jnp.where(holds, jnp.maximum(peak, new_biased), peak)
    shrink = [jnp.exp(p - peak) for p in peaks]
    new_weight = jnp.where(holds, jnp.exp(new_biased - peak), 0.0)
    weight_sum = sum(s * f for s, f in zip(sums, shrink)) + new_weight

    found = [jnp.zeros((rows, 128), f32) for _ in SEGMENTS]

    def weigh(segment, q):
        low, high = SEGMENTS[segment]
        four = jnp.concatenate([packed[2 * q + i, low:high] for i in range(2)], axis=1)
        out = jnp.dot(weights[:, low:high], four, preferred_element_type=f32)
        for i in range(2):
            pair = 4 * q + 2 * i
            found[segment] = found[segment] + jnp.where(
                row_of == pair + side, out[:, 128 * i : 128 * (i + 1)], 0.0
            )

    def joined():
        values = jnp.where(lane_of < head, 0.0, new_weight.astype(bf16).astype(f32) * new_rows)
        for f, v in zip(shrink, found):
            values = values + f * v
        return values + pltpu.roll(values, head, 1)

    quads = batch // 4
    last = len(SEGMENTS) - 1
    for segment in range(last):
        for q in range(quads):
            weigh(segment, q)
    for q in range(0, MID):
        weigh(last, q)

    diagonal = iota((rows, 128), 0) == lane_of

    def as_row(column):
        return jnp.sum(jnp.where(diagonal, column, 0.0), axis=0, keepdims=True)

    sub = iota((4, 128), 0)
    anchor = jnp.where(holds, cum_query, 0.0)
    stat_x[kv_index] = jnp.where(
        sub == 0, as_row(peak), jnp.where(sub == 1, as_row(weight_sum), as_row(anchor))
    )
    stat_all = exchange(stat_x, (kv_index, kv_offsets))


    for q in range(MID, quads // 2):
        weigh(last, q)

    half_lane = iota((half, 128), 1)

    def paired(column, part):
        found = []
        for h in range(0, heads, 2):
            low, high = h * batch + part * half, (h + 1) * batch + part * half
            found.append(jnp.where(half_lane < head, column[low : low + half], column[high : high + half]))
        return jnp.concatenate(found, axis=0)

    val_x[0, kv_index] = paired(joined(), 0).astype(bf16)
    for q in range(quads // 2, SEND):
        weigh(last, q)
    val_all = [exchange(val_x.at[0], (kv_index, kv_offsets))]
    for q in range(SEND, quads):
        weigh(last, q)
    val_x[1, kv_index] = paired(joined(), 1).astype(bf16)
    val_all.append(exchange(val_x.at[1], (kv_index, kv_offsets)))

    stat_all.wait_recv()
    peaks = stat_x[:, 0, :]
    peak = jnp.max(peaks, axis=0, keepdims=True)
    factors = jnp.exp(peaks - peak)
    weight_sum = jnp.sum(stat_x[:, 1, :] * factors, axis=0, keepdims=True)
    logs = peak + jnp.log(weight_sum) + jnp.sum(stat_x[:, 2, :], axis=0, keepdims=True)
    factors = factors / weight_sum
    log_weight[...] = jnp.concatenate([logs[:, h * batch : (h + 1) * batch] for h in range(heads)], axis=0)
    columns = factors.T
    out_all = []
    for part in range(2):
        for k in range(n_kv):
            scale[part, k] = paired(columns[:, k : k + 1], part)
        val_all[part].wait_recv()
        acc = val_x[part, 0].astype(f32) * scale[part, 0]
        for k in range(1, n_kv):
            acc = acc + val_x[part, k].astype(f32) * scale[part, k]
        attended = jnp.concatenate([acc[i * half : (i + 1) * half] for i in range(heads // 2)], axis=1)
        part_out = jnp.dot(attended.astype(bf16), wo_v[...], preferred_element_type=f32)
        out_x[part, at[2]] = part_out.astype(bf16)
        out_all.append(exchange(out_x.at[part], (at[2], tp_offsets)))
    for part in range(2):
        out_all[part].wait_recv()
        acc = out_x[part, 0].astype(f32)
        for k in range(1, n_tp):
            acc = acc + out_x[part, k].astype(f32)
        mixed[part * half : (part + 1) * half] = acc.astype(bf16)
    for every in sent:
        every.wait_send()


def store(mixed, log_weight, mixed_out, log_out, sem):
    copies = [
        pltpu.make_async_copy(mixed, mixed_out, sem.at[0]),
        pltpu.make_async_copy(log_weight, log_out, sem.at[1]),
    ]
    for copy in copies:
        copy.start()
    for copy in copies:
        copy.wait()


def shards(*args):
    (tokens, gain, w_query, w_key, w_value, gate_w, gate_bias, cache, cum, lengths, w_out) = args
    n_kv0, n_kv1, n_tp = (lax.axis_size(a) for a in ("kv_0", "kv_1", "tp"))
    n_kv = n_kv0 * n_kv1
    batch, cols = tokens.shape
    span, head = cache.shape[1], cache.shape[3] // 2
    heads = cum.shape[1]
    rows = heads * batch
    half = batch // 2
    anywhere = pl.BlockSpec(memory_space=pl.ANY)
    near = pl.BlockSpec(memory_space=pltpu.VMEM)
    mixed, logs = pl.pallas_call(
        functools.partial(kernel, n_kv0, n_kv1, n_tp),
        out_shape=(
            pltpu.VMEM((batch, w_out.shape[1]), bf16),
            pltpu.VMEM((heads, batch), f32),
        ),
        in_specs=[anywhere] * len(args),
        out_specs=(near, near),
        scratch_shapes=[
            pltpu.VMEM((batch, cols), bf16),
            pltpu.VMEM((1, cols), f32),
            pltpu.VMEM(w_query.shape, bf16),
            pltpu.VMEM((2 * head, cols), bf16),
            pltpu.VMEM((128, cols), bf16),
            pltpu.VMEM(w_out.shape, bf16),
            pltpu.SMEM(gate_bias.shape, f32),
            pltpu.SMEM(lengths.shape, jnp.int32),
            pltpu.VMEM((batch, span, 2 * head), bf16),
            pltpu.VMEM(cum.shape, f32),
            pltpu.VMEM((batch * head, span), bf16),
            pltpu.VMEM((batch // 2, span, 2 * head), bf16),
            pltpu.VMEM((rows, span), f32),
            pltpu.VMEM((rows, span), f32),
            pltpu.VMEM((rows, span), bf16),
            pltpu.VMEM((n_kv0 + n_kv1, half, heads * head + 128 + 2 * head), bf16),
            pltpu.VMEM((n_kv0 + n_kv1, half, heads * head + 128 + 2 * head), bf16),
            pltpu.VMEM((2, n_kv, rows // 4, 2 * head), bf16),
            pltpu.VMEM((n_kv, 4, rows), f32),
            pltpu.VMEM((2, n_kv, rows // 4, 2 * head), f32),
            pltpu.VMEM((2, n_tp, half, w_out.shape[1]), bf16),
            pltpu.SemaphoreType.DMA((7,)),
            pltpu.SemaphoreType.DMA((1,)),
            pltpu.SemaphoreType.DMA((7,)),
        ],
        compiler_params=pltpu.CompilerParams(
            collective_id=0, has_side_effects=True, vmem_limit_bytes=60 * 1024 * 1024
        ),
    )(
        tokens,
        gain.reshape(1, cols),
        w_query,
        w_key.T,
        w_value.T,
        gate_w.T,
        gate_bias,
        cache.reshape(batch, span, 2 * head),
        cum,
        lengths,
        w_out,
    )
    mixed, logs = pl.pallas_call(
        store,
        out_shape=(jax.ShapeDtypeStruct(mixed.shape, bf16), jax.ShapeDtypeStruct(logs.shape, f32)),
        in_specs=(near, near),
        out_specs=(anywhere, anywhere),
        scratch_shapes=[pltpu.SemaphoreType.DMA((2,))],
        compiler_params=pltpu.CompilerParams(vmem_limit_bytes=1024 * 1024),
    )(mixed, logs)
    return mixed, logs.T


def solution(mesh):
    torus = Mesh(mesh.devices.reshape(4, 4, mesh.shape["tp"]), ("kv_0", "kv_1", "tp"))
    placed = (
        P(None, KV),
        P(KV),
        P(KV, "tp"),
        P(KV, "tp"),
        P(KV, "tp"),
        P(),
        P("tp"),
        P(None, KV, "tp", None),
        P(None, "tp", KV),
        P(),
        P("tp", KV),
    )
    return jax.shard_map(
        shards, mesh=torus, in_specs=placed, out_specs=(P(None, KV), P(None, "tp")), check_vma=False
    )
```

```python
import functools
import itertools

import jax
import jax.numpy as jnp
from jax import lax
from jax.experimental import pallas as pl
from jax.experimental.pallas import tpu as pltpu
from jax.sharding import Mesh
from jax.sharding import PartitionSpec as P

KV = ("kv_0", "kv_1")
MESH = pl.DeviceIdType.MESH
NT = (((1,), (1,)), ((), ()))
norm_eps = 1e-05
masked_floor = -1e30
empty_peak = -1e29
SEGMENTS = ((0, 512), (512, 1024), (1024, 1280))
WIDEST = 640
MID, SEND = 4, 6
EARLY = 1
f32, bf16 = jnp.float32, jnp.bfloat16


def iota(shape, axis):
    return lax.broadcasted_iota(jnp.int32, shape, axis)


def pairwise(terms):
    while len(terms) > 1:
        terms = [sum(terms[k + 1 : k + 2], terms[k]) for k in range(0, len(terms), 2)]
    return terms[0]


def hops(offset, sizes):
    return sum(min(o, n - o) for o, n in zip(offset, sizes))


def cuts(low, high):
    steps = -(-(high - low) // WIDEST)
    step = -(-(high - low) // steps // 128) * 128
    return [slice(k, min(k + step, high)) for k in range(low, high, step)]


def kernel(
    n_kv0,
    n_kv1,
    n_tp,
    tokens,
    gain,
    w_query,
    w_key,
    w_value,
    gate_rows,
    gate_bias,
    cache,
    cum,
    lengths,
    w_out,
    mixed,
    log_weight,
    tok_v,
    gain_v,
    wq_v,
    wkv_v,
    wg_v,
    wo_v,
    bias_s,
    len_s,
    cache_v,
    cum_v,
    keys_t,
    packed,
    cum_neg,
    biased,
    weights,
    query_1,
    query_2,
    val_x,
    stat_x,
    scale,
    out_x,
    load_sem,
    send_sem,
    recv_sem,
):
    at = tuple(lax.axis_index(a) for a in ("kv_0", "kv_1", "tp"))
    sizes = (n_kv0, n_kv1, n_tp)
    n_kv = n_kv0 * n_kv1
    kv_index = at[0] * n_kv1 + at[1]
    batch, span = cache.shape[0], cache.shape[1]
    cols = tokens.shape[1]
    heads = cum.shape[1]
    head = cache.shape[2] // 2
    rows = heads * batch
    width = cols * n_kv
    n_gates = gate_rows.shape[0]

    def load(number, src, dst):
        copy = pltpu.make_async_copy(src, dst, load_sem.at[number])
        copy.start()
        return copy

    kv_offsets = [(a, b, 0) for a in range(n_kv0) for b in range(n_kv1) if a or b]
    tp_offsets = [(0, 0, c) for c in range(1, n_tp)]
    axis_offsets = ([(a, 0, 0) for a in range(1, n_kv0)], [(0, b, 0) for b in range(1, n_kv1)])
    for offsets in (kv_offsets, tp_offsets, *axis_offsets):
        offsets.sort(key=lambda o: (-hops(o, sizes), -sum(1 for c in o if c)))

    def moved(p, o, n):
        return jnp.where(p + o >= n, p + o - n, p + o) if o else p

    def peer(offset, sign=1):
        return tuple(moved(p, o if sign > 0 else (n - o) % n, n) for p, o, n in zip(at, offset, sizes))

    barrier = pltpu.get_barrier_semaphore()
    near_offsets = axis_offsets[0] + axis_offsets[1] + tp_offsets
    near_offsets.sort(key=lambda o: -hops(o, sizes))
    for offset in near_offsets:
        pl.semaphore_signal(barrier, inc=1, device_id=peer(offset), device_id_type=MESH)

    mine = gate_rows.at[:, pl.ds(pl.multiple_of(kv_index * cols, cols), cols)]
    small = [load(0, tokens, tok_v), load(0, gain, gain_v), load(0, w_query, wq_v)]
    small += [load(0, mine, wg_v.at[pl.ds(0, n_gates)])]
    small_new = [load(1, w_key, wkv_v.at[pl.ds(0, head)]), load(1, w_value, wkv_v.at[pl.ds(head, head)])]

    scalar_loads = [load(1, lengths, len_s), load(1, gate_bias, bias_s)]
    cum_load = load(2, cum, cum_v)
    wo_load = load(2, w_out, wo_v)
    blocks = 4
    block = batch // blocks

    def cache_copy(k):
        part = pl.ds(k * block, block)
        return pltpu.make_async_copy(cache.at[part], cache_v.at[part], load_sem.at[3 + k])

    for k in range(blocks):
        cache_copy(k).start()

    numbers = itertools.count()
    sent = []

    def exchange(buffer, *ways):
        number = next(numbers)
        copies = 0
        for me, offsets in ways:
            for offset in offsets:
                copies += 1
                pltpu.make_async_remote_copy(
                    src_ref=buffer.at[me],
                    dst_ref=buffer.at[me],
                    send_sem=send_sem.at[0],
                    recv_sem=recv_sem.at[number],
                    device_id=peer(offset),
                    device_id_type=MESH,
                ).start()
        others = buffer.at[pl.ds(0, copies)]
        every = pltpu.make_async_remote_copy(
            src_ref=others,
            dst_ref=others,
            send_sem=send_sem.at[0],
            recv_sem=recv_sem.at[number],
            device_id=peer(ways[0][1][0]),
            device_id_type=MESH,
        )
        sent.append(every)
        return every

    first_slots = (at[1], n_kv1 + at[0])
    first_ways = tuple(zip(first_slots, (axis_offsets[1], axis_offsets[0])))
    second_slots = (at[0], n_kv0 + at[1])
    second_ways = tuple(zip(second_slots, axis_offsets))

    def total(buffer, low, high):
        return pairwise([buffer[k].astype(f32) for k in range(low, high)])

    wg_v[n_gates:, :] = jnp.zeros((wg_v.shape[0] - n_gates, cols), bf16)
    for copy in small:
        copy.wait()
    tokens_f = tok_v[...].astype(f32)
    squares = jnp.sum(tokens_f * tokens_f, axis=1, keepdims=True)
    normed = (tokens_f * gain_v[...]).astype(bf16)
    lane = iota((batch, 128), 1)
    half = batch // 2
    part_query = jnp.dot(normed, wq_v[...], preferred_element_type=f32).astype(bf16)
    part_gate = lax.dot_general(normed, wg_v[...], NT, preferred_element_type=f32)
    part_gate = jnp.where(lane < n_gates, part_gate, squares).astype(bf16)
    for copy in small_new + scalar_loads:
        copy.wait()
    part_new = lax.dot_general(normed, wkv_v[...], NT, preferred_element_type=f32).astype(bf16)
    new_at = heads * head + 128
    for part in range(2):
        chunk = slice(part * half, (part + 1) * half)
        query_1[first_slots[part], :, new_at:] = part_new[chunk]
        query_1[first_slots[part], :, : heads * head] = part_query[chunk]
        query_1[first_slots[part], :, heads * head : new_at] = part_gate[chunk]

    pl.semaphore_wait(barrier, len(near_offsets))
    query_all = exchange(query_1, *first_ways)
    cum_load.wait()
    wo_load.wait()
    first_pos = kv_index * span
    length_rows = jnp.zeros((batch, 128), jnp.int32)
    for b in range(batch):
        length_rows = jnp.where(iota((batch, 128), 0) == b, len_s[b], length_rows)
    length_col = length_rows[:, :1] - first_pos
    last_parts = []
    for h in range(heads):
        last = jnp.zeros((batch, 128), f32)
        for n in range(span // 128):
            position = iota((batch, 128), 1) + n * 128
            value = cum_v[:, h, n * 128 : (n + 1) * 128]
            cum_neg[h * batch : (h + 1) * batch, n * 128 : (n + 1) * 128] = jnp.where(
                position < length_col, -value, masked_floor
            )
            last = last + jnp.where(position == length_col - 1, value, 0.0)
        last_parts.append(jnp.sum(last, axis=1, keepdims=True))
    last_cum = jnp.concatenate(last_parts, axis=0)
    holds = (length_col > 0) & (length_col <= span)
    holds = jnp.concatenate([jnp.where(holds, 1, 0)] * heads, axis=0) > 0

    column = iota((4 * head, 2 * head), 1)
    chosen = jnp.where(column < head, column + head, column + 2 * head)
    chooser = jnp.where(iota((4 * head, 2 * head), 0) == chosen, 1.0, 0.0).astype(bf16)

    def prepare(k):
        cache_copy(k).wait()

        def one(j, carry):
            b = 2 * (k * block // 2 + j)
            pair = jnp.concatenate([cache_v[b], cache_v[b + 1]], axis=1)
            packed[k * block // 2 + j] = jnp.dot(pair, chooser, preferred_element_type=f32).astype(bf16)
            for i in range(2):
                keys_t[pl.ds(pl.multiple_of((b + i) * head, head), head), :] = cache_v[b + i].T[:head]
            return carry

        for j in range(block//2): one(j,0)

    for k in range(EARLY):
        prepare(k)

    query_all.wait_recv()
    query_2[second_slots[0]] = total(query_1, 0, n_kv1).astype(bf16)
    query_2[second_slots[1]] = total(query_1, n_kv1, n_kv1 + n_kv0).astype(bf16)
    query_all = exchange(query_2, *second_ways)
    for k in range(EARLY, blocks):
        prepare(k)
    query_all.wait_recv()
    sums = jnp.concatenate([total(query_2, 0, n_kv0), total(query_2, n_kv0, n_kv0 + n_kv1)], axis=0)
    sum_query, gates, sum_new = sums[:, : heads * head], sums[:, heads * head : new_at], sums[:, new_at:]
    total_squares = gates[:, n_gates : n_gates + 1]
    row_scale = lax.rsqrt(total_squares / width + norm_eps)
    query = sum_query.astype(bf16).astype(f32)
    log_gate = []
    for h in range(heads):
        pick = at[2] * heads + h
        logit = jnp.sum(jnp.where(lane == pick, gates, 0.0), axis=1, keepdims=True)
        logit = row_scale * logit + bias_s[h]
        log_gate.append(jnp.minimum(logit, 0.0) - jnp.log1p(jnp.exp(-jnp.abs(logit))))
    cum_query = last_cum + jnp.concatenate(log_gate, axis=0)

    doubled = []
    for pair in range(heads // 2):
        two = query[:, pair * 128 : (pair + 1) * 128]
        turned = pltpu.roll(two, 64, 1)
        doubled.append(jnp.where(lane < head, two, turned))
        doubled.append(jnp.where(lane < head, turned, two))
    doubled = jnp.concatenate(doubled, axis=0)
    row_of = iota((rows, 128), 0) % batch
    lane_of = iota((rows, 128), 1)
    side = jnp.where(lane_of < head, 0, 1)
    inv_root = head ** (-0.5)
    scaled = doubled
    row_factor = jnp.concatenate([row_scale] * heads, axis=0) * inv_root
    spread = jnp.concatenate(
        [jnp.where(row_of == 2 * p + side, scaled, 0.0).astype(bf16) for p in range(batch // 2)], axis=1
    )

    peaks, sums = [], []
    for low, high in SEGMENTS:
        top = jnp.full((rows, 128), masked_floor, f32)
        for cut in cuts(low, high):
            score = jnp.dot(spread, keys_t[:, cut], preferred_element_type=f32) * row_factor + cum_neg[:, cut]
            biased[:, cut] = score
            for k in range(score.shape[1] // 128):
                top = jnp.maximum(top, score[:, k * 128 : (k + 1) * 128])
        top = jnp.maximum(jnp.max(top, axis=1, keepdims=True), empty_peak)
        part_sum = jnp.zeros((rows, 128), f32)
        for k in range(low, high, 128):
            weight = jnp.exp(biased[:, k : k + 128] - top)
            part_sum = part_sum + weight
            weights[:, k : k + 128] = weight.astype(bf16)
        peaks.append(top)
        sums.append(jnp.sum(part_sum, axis=1, keepdims=True))

    new_rows = sum_new
    new_rows = (row_scale * new_rows).astype(bf16).astype(f32)
    new_rows = jnp.concatenate([new_rows] * heads, axis=0)
    new_biased = (
        jnp.sum(jnp.where(lane_of < head, doubled * new_rows, 0.0), axis=1, keepdims=True) * row_factor
        - cum_query
    )

    peak = functools.reduce(jnp.maximum, peaks)
    peak = jnp.where(holds, jnp.maximum(peak, new_biased), peak)
    shrink = [jnp.exp(p - peak) for p in peaks]
    new_weight = jnp.where(holds, jnp.exp(new_biased - peak), 0.0)
    weight_sum = sum(s * f for s, f in zip(sums, shrink)) + new_weight

    found = [jnp.zeros((rows, 128), f32) for _ in SEGMENTS]

    def weigh(segment, q):
        low, high = SEGMENTS[segment]
        four = jnp.concatenate([packed[2 * q + i, low:high] for i in range(2)], axis=1)
        out = jnp.dot(weights[:, low:high], four, preferred_element_type=f32)
        for i in range(2):
            pair = 4 * q + 2 * i
            found[segment] = found[segment] + jnp.where(
                row_of == pair + side, out[:, 128 * i : 128 * (i + 1)], 0.0
            )

    def joined():
        values = jnp.where(lane_of < head, 0.0, new_weight.astype(bf16).astype(f32) * new_rows)
        for f, v in zip(shrink, found):
            values = values + f * v
        return values + pltpu.roll(values, head, 1)

    quads = batch // 4
    last = len(SEGMENTS) - 1
    for segment in range(last):
        for q in range(quads):
            weigh(segment, q)
    for q in range(0, MID):
        weigh(last, q)

    diagonal = iota((rows, 128), 0) == lane_of

    def as_row(column):
        return jnp.sum(jnp.where(diagonal, column, 0.0), axis=0, keepdims=True)

    sub = iota((4, 128), 0)
    anchor = jnp.where(holds, cum_query, 0.0)
    stat_x[kv_index] = jnp.where(
        sub == 0, as_row(peak), jnp.where(sub == 1, as_row(weight_sum), as_row(anchor))
    )
    stat_all = exchange(stat_x, (kv_index, kv_offsets))


    for q in range(MID, quads // 2):
        weigh(last, q)

    half_lane = iota((half, 128), 1)

    def paired(column, part):
        found = []
        for h in range(0, heads, 2):
            low, high = h * batch + part * half, (h + 1) * batch + part * half
            found.append(jnp.where(half_lane < head, column[low : low + half], column[high : high + half]))
        return jnp.concatenate(found, axis=0)

    val_x[0, kv_index] = paired(joined(), 0).astype(bf16)
    for q in range(quads // 2, SEND):
        weigh(last, q)
    val_all = [exchange(val_x.at[0], (kv_index, kv_offsets))]
    for q in range(SEND, quads):
        weigh(last, q)
    val_x[1, kv_index] = paired(joined(), 1).astype(bf16)
    val_all.append(exchange(val_x.at[1], (kv_index, kv_offsets)))

    stat_all.wait_recv()
    peaks = stat_x[:, 0, :]
    peak = jnp.max(peaks, axis=0, keepdims=True)
    factors = jnp.exp(peaks - peak)
    weight_sum = jnp.sum(stat_x[:, 1, :] * factors, axis=0, keepdims=True)
    logs = peak + jnp.log(weight_sum) + jnp.sum(stat_x[:, 2, :], axis=0, keepdims=True)
    factors = factors / weight_sum
    log_weight[...] = jnp.concatenate([logs[:, h * batch : (h + 1) * batch] for h in range(heads)], axis=0)
    columns = factors.T
    out_all = []
    for part in range(2):
        for k in range(n_kv):
            scale[part, k] = paired(columns[:, k : k + 1], part)
        val_all[part].wait_recv()
        acc = pairwise([val_x[part, k].astype(f32) * scale[part, k] for k in range(n_kv)])
        attended = jnp.concatenate([acc[i * half : (i + 1) * half] for i in range(heads // 2)], axis=1)
        part_out = jnp.dot(attended.astype(bf16), wo_v[...], preferred_element_type=f32)
        out_x[part, at[2]] = part_out.astype(bf16)
        out_all.append(exchange(out_x.at[part], (at[2], tp_offsets)))
    for part in range(2):
        out_all[part].wait_recv()
        acc = pairwise([out_x[part, k].astype(f32) for k in range(n_tp)])
        mixed[part * half : (part + 1) * half] = acc.astype(bf16)
    for every in sent:
        every.wait_send()


def store(mixed, log_weight, mixed_out, log_out, sem):
    copies = [
        pltpu.make_async_copy(mixed, mixed_out, sem.at[0]),
        pltpu.make_async_copy(log_weight, log_out, sem.at[1]),
    ]
    for copy in copies:
        copy.start()
    for copy in copies:
        copy.wait()


def shards(*args):
    (tokens, gain, w_query, w_key, w_value, gate_w, gate_bias, cache, cum, lengths, w_out) = args
    n_kv0, n_kv1, n_tp = (lax.axis_size(a) for a in ("kv_0", "kv_1", "tp"))
    n_kv = n_kv0 * n_kv1
    batch, cols = tokens.shape
    span, head = cache.shape[1], cache.shape[3] // 2
    heads = cum.shape[1]
    rows = heads * batch
    half = batch // 2
    anywhere = pl.BlockSpec(memory_space=pl.ANY)
    near = pl.BlockSpec(memory_space=pltpu.VMEM)
    mixed, logs = pl.pallas_call(
        functools.partial(kernel, n_kv0, n_kv1, n_tp),
        out_shape=(
            pltpu.VMEM((batch, w_out.shape[1]), bf16),
            pltpu.VMEM((heads, batch), f32),
        ),
        in_specs=[anywhere] * len(args),
        out_specs=(near, near),
        scratch_shapes=[
            pltpu.VMEM((batch, cols), bf16),
            pltpu.VMEM((1, cols), f32),
            pltpu.VMEM(w_query.shape, bf16),
            pltpu.VMEM((2 * head, cols), bf16),
            pltpu.VMEM((128, cols), bf16),
            pltpu.VMEM(w_out.shape, bf16),
            pltpu.SMEM(gate_bias.shape, f32),
            pltpu.SMEM(lengths.shape, jnp.int32),
            pltpu.VMEM((batch, span, 2 * head), bf16),
            pltpu.VMEM(cum.shape, f32),
            pltpu.VMEM((batch * head, span), bf16),
            pltpu.VMEM((batch // 2, span, 2 * head), bf16),
            pltpu.VMEM((rows, span), f32),
            pltpu.VMEM((rows, span), f32),
            pltpu.VMEM((rows, span), bf16),
            pltpu.VMEM((n_kv0 + n_kv1, half, heads * head + 128 + 2 * head), bf16),
            pltpu.VMEM((n_kv0 + n_kv1, half, heads * head + 128 + 2 * head), bf16),
            pltpu.VMEM((2, n_kv, rows // 4, 2 * head), bf16),
            pltpu.VMEM((n_kv, 4, rows), f32),
            pltpu.VMEM((2, n_kv, rows // 4, 2 * head), f32),
            pltpu.VMEM((2, n_tp, half, w_out.shape[1]), bf16),
            pltpu.SemaphoreType.DMA((7,)),
            pltpu.SemaphoreType.DMA((1,)),
            pltpu.SemaphoreType.DMA((7,)),
        ],
        compiler_params=pltpu.CompilerParams(
            collective_id=0, has_side_effects=True, vmem_limit_bytes=60 * 1024 * 1024
        ),
    )(
        tokens,
        gain.reshape(1, cols),
        w_query,
        w_key.T,
        w_value.T,
        gate_w.T,
        gate_bias,
        cache.reshape(batch, span, 2 * head),
        cum,
        lengths,
        w_out,
    )
    mixed, logs = pl.pallas_call(
        store,
        out_shape=(jax.ShapeDtypeStruct(mixed.shape, bf16), jax.ShapeDtypeStruct(logs.shape, f32)),
        in_specs=(near, near),
        out_specs=(anywhere, anywhere),
        scratch_shapes=[pltpu.SemaphoreType.DMA((2,))],
        compiler_params=pltpu.CompilerParams(vmem_limit_bytes=1024 * 1024),
    )(mixed, logs)
    return mixed, logs.T


def solution(mesh):
    torus = Mesh(mesh.devices.reshape(4, 4, mesh.shape["tp"]), ("kv_0", "kv_1", "tp"))
    placed = (
        P(None, KV),
        P(KV),
        P(KV, "tp"),
        P(KV, "tp"),
        P(KV, "tp"),
        P(),
        P("tp"),
        P(None, KV, "tp", None),
        P(None, "tp", KV),
        P(),
        P("tp", KV),
    )
    return jax.shard_map(
        shards, mesh=torus, in_specs=placed, out_specs=(P(None, KV), P(None, "tp")), check_vma=False
    )
```
